32 devices in a mesh: sp: 8 (over z, y), tp: 4 (over x, core).
Axes of the slice: x: 2, y: 2, z: 4, core: 2. Of those that a mesh axis runs over, the one named last changes fastest.
Arguments:
- values_in: bfloat16 [4, 8192, 1024], P(None, 'sp', 'tp'), may hold values from -6 to 6
- gates_in: bfloat16 [4, 8192, 1024], P(None, 'sp', 'tp'), may hold values from -8 to 8
- conv_taps: bfloat16 [31, 1024], P(None, 'tp'), may hold values from -3 to 3
- conv_bias: bfloat16 [1024], P('tp'), may hold values from -3 to 3
- norm_gain: bfloat16 [1024], P('tp'), may hold values from 0.099609375 to 1.8984375
- out_weight: bfloat16 [1024, 4096], P('tp'), may hold values from -0.1875 to 0.1875
- out_grad: bfloat16 [4, 8192, 4096], P(None, 'sp'), may hold values from -1.5 to 1.5
Outputs:
- values_grad: bfloat16 [4, 8192, 1024], P(None, 'sp', 'tp')
- gates_grad: bfloat16 [4, 8192, 1024], P(None, 'sp', 'tp')
- taps_grad: float32 [31, 1024], P(None, 'tp')
- gain_grad: float32 [1024], P('tp')
- bias_grad: float32 [1024], P('tp')
- weight_grad: float32 [1024, 4096], P(('tp', 'sp'))
The draws below stay inside these ranges and needn't reach their ends.
All inputs are finite; a program needn't handle non-finite values.
Results may differ from the reference program's by a relative error of at most 0.0048.
Values may be sent and summed in bfloat16 or wider, within the bound.
A program may use at most 128 MiB of HBM per device.

```python
import jax
import jax.numpy as jnp
from jax import lax

D = 4096
C = 1024
K = 31
SEQS = 4
TOKENS = 8192


def draw_conv_taps(key, part):
    normal_key, scale_key = jax.random.split(jax.random.fold_in(key, 7))
    group_count = C // 64
    scales = jnp.exp(jax.random.uniform(scale_key, (group_count,), jnp.float32, -1.2, 1.2))
    scales = jnp.repeat(scales, 64)
    noise = jax.random.normal(normal_key, (K, C), jnp.float32)
    noise = jnp.clip(noise, -4.0, 4.0)
    return (noise * scales[None, :] * K ** (-0.5)).astype(jnp.bfloat16)


def block_levels(key, shape, cuts, smallest, largest):
    def one(dim, blocks):
        draws = jax.random.uniform(jax.random.fold_in(jax.random.fold_in(key, 6), dim), (blocks,), jnp.float32, smallest / len(cuts), largest / len(cuts))
        return jnp.repeat(jnp.exp(draws), shape[dim] // blocks).reshape((-1,) + (1,) * (len(shape) - dim - 1))

    level = one(*cuts[0])
    for cut in cuts[1:]:
        level = level * one(*cut)
    return level


def normal_values(key, shape, spread, reach, cuts=(), held_as=jnp.bfloat16):
    level = block_levels(key, shape, cuts, -0.22, 0.18) if cuts else 1.0
    result = jax.random.normal(key, shape, jnp.float32) * spread * level
    return jnp.minimum(jnp.maximum(result, -reach), reach).astype(held_as)


def setup_inputs(seed: int = 0) -> dict:
    key_of = jax.random.split(jax.random.key(seed), 8)
    values_in = normal_values(key_of[0], (SEQS, TOKENS, C), 1.0, 6.0, ((1, 8), (2, 4)))
    gates_in = normal_values(key_of[1], (SEQS, TOKENS, C), 1.5, 8.0, ((1, 8), (2, 4)))
    conv_taps = draw_conv_taps(jax.random.fold_in(key_of[7], 71), 0)
    conv_bias = normal_values(key_of[3], (C,), 0.5, 3.0, ((0, 4),))
    norm_gain = jnp.clip(1.0 + 0.18 * jax.random.normal(key_of[4], (C,), jnp.float32), 0.099609375, 1.8984375).astype(jnp.bfloat16)
    out_weight = normal_values(key_of[5], (C, D), C ** -0.5, 0.1875, ((0, 4),))
    out_grad = normal_values(key_of[6], (SEQS, TOKENS, D), 0.25, 1.5, ((1, 8),))
    return {"values_in": values_in, "gates_in": gates_in, "conv_taps": conv_taps, "conv_bias": conv_bias, "norm_gain": norm_gain, "out_weight": out_weight, "out_grad": out_grad}


EPS = 1e-05

def reference(values_in, gates_in, conv_taps, conv_bias, norm_gain, out_weight, out_grad):
    sig = jax.nn.sigmoid(gates_in.astype(jnp.float32))
    gated = (values_in.astype(jnp.float32) * sig).astype(jnp.bfloat16)
    tap_rows = conv_taps.astype(jnp.float32)
    length = gated.shape[1]
    padded = jnp.pad(gated.astype(jnp.float32), ((0, 0), (K - 1, 0), (0, 0)))
    conv = jnp.zeros(gated.shape, jnp.float32) + conv_bias.astype(jnp.float32)
    for tap_index in range(K):
        conv = conv + tap_rows[tap_index] * padded[:, tap_index:tap_index + length]
    channel_mean = lax.optimization_barrier(jnp.mean(conv, axis=-1, keepdims=True))
    centered = conv - channel_mean
    variance = lax.optimization_barrier(jnp.mean(centered * centered, axis=-1, keepdims=True))
    inverse = lax.rsqrt(variance + EPS)
    normed = centered * inverse
    gain = norm_gain.astype(jnp.float32)
    scaled = normed * gain
    swished = jax.nn.silu(scaled).astype(jnp.bfloat16)
    flat_grad = out_grad.reshape(-1, D)
    weight_grad = jnp.dot(swished.reshape(-1, C).T, flat_grad, preferred_element_type=jnp.float32)
    swish_grad = jnp.dot(flat_grad, out_weight.T, preferred_element_type=jnp.float32).reshape(gated.shape)
    scaled_sig = jax.nn.sigmoid(scaled)
    scaled_grad = swish_grad * scaled_sig * (1.0 + scaled * (1.0 - scaled_sig))
    gain_grad = lax.optimization_barrier(jnp.sum(scaled_grad * normed, axis=(0, 1)))
    normed_grad = scaled_grad * gain
    conv_grad = inverse * (normed_grad - lax.optimization_barrier(jnp.mean(normed_grad, axis=-1, keepdims=True)) - normed * lax.optimization_barrier(jnp.mean(normed_grad * normed, axis=-1, keepdims=True)))
    bias_grad = lax.optimization_barrier(jnp.sum(conv_grad, axis=(0, 1)))
    taps_grad = jnp.stack([lax.optimization_barrier(jnp.sum(conv_grad * padded[:, tap_index:tap_index + length], axis=(0, 1))) for tap_index in range(K)])
    padded_grad = jnp.pad(conv_grad, ((0, 0), (0, K - 1), (0, 0)))
    gated_grad = jnp.zeros(gated.shape, jnp.float32)
    for tap_index in range(K):
        begin = K - 1 - tap_index
        gated_grad = gated_grad + tap_rows[tap_index] * padded_grad[:, begin:begin + length]
    values_grad = (gated_grad * sig).astype(jnp.bfloat16)
    gates_grad = (gated_grad * values_in.astype(jnp.float32) * sig * (1.0 - sig)).astype(jnp.bfloat16)
    return (values_grad, gates_grad, taps_grad, gain_grad, bias_grad, weight_grad)
```

```python
import functools

import jax
import jax.numpy as jnp
import numpy as np
from jax import lax
from jax.experimental import pallas as pl
from jax.experimental.pallas import tpu as pltpu
from jax.sharding import PartitionSpec as P

K = 31
EPS = 1e-05
HALO = 32
PAIR = 2
LANES = 128
SPAN = 256
STEP = SPAN - HALO
F32 = jnp.float32
BF16 = jnp.bfloat16
VMEM_LIMIT = 64 * 1024 * 1024 - 64 * 1024

FWD, GRAD, INV, CONV, TAPF, TAPI = 0, 512, 1024, 1536, 1984, 2496
TABLE_ROWS = 2560


def transform_table():
    row = np.arange(SPAN)
    freq = 8 * (row // 16) + row % 8
    angle = 2 * np.pi * (freq[:, None] + 0.5) * np.arange(SPAN)[None] / SPAN
    fwd = np.where((row // 8 % 2 == 0)[:, None], np.cos(angle), -np.sin(angle))
    inv = fwd.T * (2 / SPAN)
    grad = np.zeros((SPAN, SPAN))
    grad[:, :STEP] = fwd[:, HALO:]
    tap_fwd = np.zeros((SPAN, SPAN))
    tap_fwd[:, :K] = fwd[:, K - 1 :: -1]
    tap_inv = np.zeros((32, SPAN))
    tap_inv[:K] = inv[K - 1 :: -1]
    parts = []
    for whole_part in (fwd, grad, inv, inv[HALO:], tap_fwd, tap_inv):
        high = whole_part.astype(BF16)
        parts += [high, (whole_part - high.astype(np.float64)).astype(BF16)]
    return np.concatenate(parts)


def sigmoid(x):
    return 0.5 * jnp.tanh(0.5 * x) + 0.5


def peer_id(axis, distance):
    devices = lax.axis_size(axis)
    return {axis: lax.rem(lax.axis_index(axis) + distance, devices)}


def greet(pairs):
    barrier = pltpu.get_barrier_semaphore()
    for axis, distance in pairs:
        pl.semaphore_signal(
            barrier, inc=1, device_id=peer_id(axis, distance),
            device_id_type=pl.DeviceIdType.MESH,
        )
    pl.semaphore_wait(barrier, len(pairs))


def remote(src, dst, send_sem, recv_sem, axis, distance):
    return pltpu.make_async_remote_copy(
        src_ref=src, dst_ref=dst, send_sem=send_sem, recv_sem=recv_sem,
        device_id=peer_id(axis, distance), device_id_type=pl.DeviceIdType.MESH,
    )


def dot(a, b):
    return jnp.dot(a, b, preferred_element_type=F32)


def lane_sums(x):
    return jnp.sum(x.T, axis=0, keepdims=True)


def row_spread(row):
    return jnp.broadcast_to(row, (LANES, LANES)).T


def split(x):
    high = x.astype(BF16)
    return high, (x - high.astype(F32)).astype(BF16)


def fused_kernel(
    total_chans, values_hbm, gates_hbm, cot_hbm, weight_hbm, table_hbm, taps_ref, bias_ref,
    gain_ref,
    spread_hbm, heads_ref, small_ref, weight_out_ref,
    values, gates, values_halo, gates_halo, cot, swished, weight_t, weight_grad, pair, onward,
    arrived, conv, grad, xpad, spectrum, high, low, grad_high, grad_low, table, tap_rows,
    tap_re, tap_im, corr_re, corr_im, heads, heads_in, sums, sums_in, stat, back, back_in,
    gain_acc, bias_acc, small, small_in,
    load_sems, cot_sems, misc_sems, out_sems, halo_send, halo_recv, sums_send, sums_recv,
    back_send, back_recv, pair_send, pair_recv, onward_send, onward_recv, head_send, head_recv,
    small_send, small_recv,
):
    seqs, tokens, chans = values.shape
    positions, width = cot.shape
    lane_blocks = chans // LANES
    chunks = tokens // LANES
    windows = spectrum.shape[0] // seqs
    blocks, rows = cot_sems.shape[0], grad.shape[1]
    seq_blocks = blocks // seqs
    block_chunks = rows // LANES
    parts = pair_send.shape[0]
    part_width = width // parts
    groups, weight_rows = pair.shape[0], pair.shape[1]
    sp_devices = lax.axis_size("sp")
    me = lax.axis_index("sp")
    inner = lax.rem(me, PAIR)
    outer = me // PAIR
    tp_peers = range(1, lax.axis_size("tp"))
    sp_peers = range(1, sp_devices)

    loads = []
    for n, (src, dst) in enumerate(((weight_hbm, swished.at[:, :width]), (table_hbm, table))):
        copy = pltpu.make_async_copy(src, dst, misc_sems.at[n])
        copy.start()
        loads.append(copy)

    def seq_loads(s):
        return [
            pltpu.make_async_copy(src.at[s], dst.at[s], load_sems.at[n, s])
            for n, (src, dst) in enumerate(((values_hbm, values), (gates_hbm, gates)))
        ]

    for s in range(seqs):
        for copy in seq_loads(s):
            copy.start()

    def cot_load(i):
        here = pl.ds(pl.multiple_of(i * rows, rows), rows)
        return pltpu.make_async_copy(cot_hbm.at[here], cot.at[here], cot_sems.at[i])

    for i in range(blocks):
        cot_load(i).start()

    greet([("tp", d) for d in tp_peers] + [("sp", d) for d in sp_peers])
    last = pl.ds(tokens - HALO, HALO)
    halo_copies = [
        remote(src.at[:, last], dst, halo_send.at[n], halo_recv.at[n], "sp", 1)
        for n, (src, dst) in enumerate(((values_hbm, values_halo), (gates_hbm, gates_halo)))
    ]
    for copy in halo_copies:
        copy.start()

    xpad[HALO + tokens :, :] = jnp.zeros((xpad.shape[0] - HALO - tokens, chans), BF16)
    for ref in (grad_high, grad_low):
        ref[tokens:, :] = jnp.zeros((ref.shape[0] - tokens, chans), BF16)
    for ref in (gain_acc, bias_acc, corr_re, corr_im, tap_rows):
        ref[...] = jnp.zeros_like(ref)
    tap_rows[:K, :] = taps_ref[...].astype(F32)
    bias = bias_ref[...].astype(F32).reshape(1, chans)
    gain = gain_ref[...].astype(F32).reshape(1, chans)

    for copy in loads:
        copy.wait()
    taps_wide = dot(table[TAPF : TAPF + 2 * SPAN], tap_rows[...].astype(BF16))
    taps_wide = taps_wide[:SPAN] + taps_wide[SPAN:]
    for q in range(SPAN // 16):
        tap_re[8 * q : 8 * q + 8, :] = taps_wide[16 * q : 16 * q + 8]
        tap_im[8 * q : 8 * q + 8, :] = taps_wide[16 * q + 8 : 16 * q + 16]

    def turn(i, carry):
        here = pl.ds(pl.multiple_of(i * 512, 512), 512)
        weight_t[here, :] = swished[:, here].T
        return carry

    lax.fori_loop(0, width // 512, turn, 0)

    def product(x, w, sign):
        for q in range(SPAN // 16):
            a, b = tap_re[8 * q : 8 * q + 8, :], tap_im[8 * q : 8 * q + 8, :]
            re, im = x[16 * q : 16 * q + 8], x[16 * q + 8 : 16 * q + 16]
            if sign > 0:
                both = (a * re - b * im, a * im + b * re)
            else:
                both = (a * re + b * im, a * im - b * re)
            here = slice(16 * q, 16 * q + 16)
            high[w, here, :], low[w, here, :] = split(jnp.concatenate(both, axis=0))

    def sums_copies(s):
        return [
            remote(sums.at[s], sums_in.at[d - 1, s], sums_send.at[d - 1, s],
                   sums_recv.at[d - 1, s], "tp", d)
            for d in tp_peers
        ]

    for copy in halo_copies:
        copy.wait()
    keep = jnp.where(me > 0, 1.0, 0.0).astype(F32)

    def gate(values_part, gates_part):
        return values_part.astype(F32) * sigmoid(gates_part.astype(F32))

    def ahead(s, carry):
        for copy in seq_loads(s):
            copy.wait()
        xpad[:HALO, :] = (gate(values_halo[s], gates_halo[s]) * keep).astype(BF16)
        for i in range(chunks):
            here = slice(i * LANES, (i + 1) * LANES)
            xpad[HALO + i * LANES : HALO + (i + 1) * LANES, :] = gate(
                values[s, here, :], gates[s, here, :]
            ).astype(BF16)
        for w in range(windows):
            x = dot(table[FWD : FWD + 2 * SPAN], xpad[w * STEP : w * STEP + SPAN, :])
            x = x[:SPAN] + x[SPAN:]
            spectrum[s * windows + w] = x.astype(BF16)
            product(x, w, 1)
        for w in range(windows):
            y = dot(table[CONV : CONV + 2 * STEP], high[w])
            y = y[:STEP] + y[STEP:] + dot(table[CONV : CONV + STEP], low[w]) + bias
            count = min(STEP, tokens - w * STEP)
            conv[s, w * STEP : w * STEP + count, :] = y[:count]
        for i in range(chunks):
            total = square = None
            for h in range(lane_blocks):
                part = conv[s, i * LANES : (i + 1) * LANES, h * LANES : (h + 1) * LANES]
                total = part if total is None else total + part
                square = part * part if square is None else square + part * part
            sums[s, 0, i : i + 1, :] = lane_sums(total)
            sums[s, 1, i : i + 1, :] = lane_sums(square)
        for copy in sums_copies(s):
            copy.start()
        return carry

    lax.fori_loop(0, seqs, ahead, 0)

    def norm(s, carry):
        total = sums[s]
        for d, copy in zip(tp_peers, sums_copies(s)):
            copy.wait()
            total = total + sums_in[d - 1, s]
        mean_rows = total[0] / total_chans
        variance = total[1] / total_chans - mean_rows * mean_rows
        inverse_rows = lax.rsqrt(variance + EPS)
        stat[s] = inverse_rows
        for i in range(chunks):
            here = slice(i * LANES, (i + 1) * LANES)
            columns = pl.ds(pl.multiple_of(s * tokens + i * LANES, LANES), LANES)
            mean = row_spread(mean_rows[i : i + 1])
            inverse = row_spread(inverse_rows[i : i + 1])
            for h in range(lane_blocks):
                lanes = slice(h * LANES, (h + 1) * LANES)
                normed = (conv[s, here, lanes] - mean) * inverse
                conv[s, here, lanes] = normed
                scaled = normed * gain[:, lanes]
                swished[lanes, columns] = (scaled * sigmoid(scaled)).T.astype(BF16)
        return carry

    lax.fori_loop(0, seqs, norm, 0)

    for i in range(blocks):
        cot_load(i).wait()

    def part_columns(c):
        return pl.ds(pl.multiple_of(c * part_width, part_width), part_width)

    def pair_copy(c):
        columns = part_columns(c)
        return remote(
            weight_grad.at[1 - inner, :, :, columns], pair.at[:, :, columns], pair_send.at[c],
            pair_recv.at[c], "sp", sp_devices + 1 - 2 * inner,
        )

    def onward_copy(d, c):
        columns = part_columns(c)
        return remote(
            onward.at[d - 1, :, columns], arrived.at[d - 1, :, columns], onward_send.at[d - 1, c],
            onward_recv.at[d - 1, c], "sp", d * PAIR,
        )

    def project(c, carry):
        columns = part_columns(c)
        result = dot(swished[:, :positions], cot[:, columns])
        for g in range(groups):
            for n in range(PAIR):
                first = (g * PAIR + n) * weight_rows
                weight_grad[n, g, :, columns] = result[first : first + weight_rows].astype(BF16)
        pair_copy(c).start()
        return carry

    lax.fori_loop(0, parts, project, 0)

    def pass_on(c):
        columns = part_columns(c)
        pair_copy(c).wait()
        for d in range(1, groups):
            target = lax.rem(outer + d, groups)
            onward[d - 1, :, columns] = (
                weight_grad[inner, target, :, columns].astype(F32)
                + pair[target, :, columns].astype(F32)
            ).astype(BF16)
        for d in range(1, groups):
            onward_copy(d, c).start()

    def back_copies(j):
        return [
            remote(back.at[j], back_in.at[d - 1, j], back_send.at[d - 1, j],
                   back_recv.at[d - 1, j], "tp", d)
            for d in tp_peers
        ]

    def multiply(j):
        here = pl.ds(pl.multiple_of(j * rows, rows), rows)
        grad[lax.rem(j, 2)] = dot(cot[here, :], weight_t[...])

    def middle(j):
        s = j // seq_blocks
        first = lax.rem(j, seq_blocks) * rows
        slot = lax.rem(j, 2)
        for i in range(block_chunks):
            here = pl.ds(pl.multiple_of(first + i * LANES, LANES), LANES)
            plain = weighted = None
            for h in range(lane_blocks):
                lanes = slice(h * LANES, (h + 1) * LANES)
                normed = conv[s, here, lanes]
                scaled = normed * gain[:, lanes]
                sig = sigmoid(scaled)
                silu = scaled * sig
                scaled_grad = grad[slot, i * LANES : (i + 1) * LANES, lanes] * (
                    sig + silu * (1.0 - sig)
                )
                normed_grad = scaled_grad * gain[:, lanes]
                values[s, here, lanes], gates[s, here, lanes] = split(normed_grad)
                term = scaled_grad * normed
                gain_acc[:, lanes] += jnp.sum(term.reshape(LANES // 8, 8, LANES), axis=0)
                term = normed_grad * normed
                plain = normed_grad if plain is None else plain + normed_grad
                weighted = term if weighted is None else weighted + term
            back[j, 0, i : i + 1, :] = lane_sums(plain)
            back[j, 1, i : i + 1, :] = lane_sums(weighted)
        for copy in back_copies(j):
            copy.start()

    multiply(0)

    def both(j, carry):
        middle(j - 1)
        multiply(j)

        @pl.when(lax.rem(j, 2) == 0)
        def _():
            pass_on(j // 2 - 1)

        return carry

    lax.fori_loop(1, blocks, both, 0)
    middle(blocks - 1)
    passed = min((blocks - 1) // 2, parts)

    def spread_copy(s):
        return pltpu.make_async_copy(conv.at[s], spread_hbm.at[s], out_sems.at[s])

    def head_copy(s):
        return remote(
            heads.at[s], heads_in.at[s], head_send.at[s], head_recv.at[s], "sp", sp_devices - 1
        )

    def behind(s, carry):
        for n in range(seq_blocks):
            for copy in back_copies(s * seq_blocks + n):
                copy.wait()
        for i in range(chunks):
            here = slice(i * LANES, (i + 1) * LANES)
            j = s * seq_blocks + i // block_chunks
            at = slice(i % block_chunks, i % block_chunks + 1)
            inverse_row = stat[s, i : i + 1, :]
            plain, weighted = back[j, 0, at, :], back[j, 1, at, :]
            for d in tp_peers:
                plain = plain + back_in[d - 1, j, 0, at, :]
                weighted = weighted + back_in[d - 1, j, 1, at, :]
            scale = inverse_row / total_chans
            inverse = row_spread(inverse_row)
            plain = row_spread(plain * scale)
            weighted = row_spread(weighted * scale)
            for h in range(lane_blocks):
                lanes = slice(h * LANES, (h + 1) * LANES)
                normed_grad = values[s, here, lanes].astype(F32) + gates[s, here, lanes].astype(
                    F32
                )
                conv_grad = inverse * normed_grad - plain - conv[s, here, lanes] * weighted
                grad_high[here, lanes], grad_low[here, lanes] = split(conv_grad)
                bias_acc[:, lanes] += jnp.sum(conv_grad.reshape(LANES // 8, 8, LANES), axis=0)
        for w in range(windows):
            here = slice(w * STEP, w * STEP + SPAN)
            g = dot(table[GRAD : GRAD + 2 * SPAN], grad_high[here, :])
            g = g[:SPAN] + g[SPAN:] + dot(table[GRAD : GRAD + SPAN], grad_low[here, :])
            x = spectrum[s * windows + w].astype(F32)
            for q in range(SPAN // 16):
                at = slice(8 * q, 8 * q + 8)
                g_re, g_im = g[16 * q : 16 * q + 8], g[16 * q + 8 : 16 * q + 16]
                x_re, x_im = x[16 * q : 16 * q + 8], x[16 * q + 8 : 16 * q + 16]
                corr_re[at, :] += g_re * x_re + g_im * x_im
                corr_im[at, :] += g_im * x_re - g_re * x_im
            product(g, w, -1)
        for w in range(windows):
            y = dot(table[INV : INV + 2 * SPAN], high[w])
            y = y[:SPAN] + y[SPAN:] + dot(table[INV : INV + SPAN], low[w])
            if w == 0:
                heads[s] = y[:HALO]
            else:
                conv[s, w * STEP - HALO : w * STEP, :] += y[:HALO]
            count = min(STEP, tokens - w * STEP)
            conv[s, w * STEP : w * STEP + count, :] = y[HALO : HALO + count]
        spread_copy(s).start()
        head_copy(s).start()

        @pl.when(passed + s < parts)
        def _():
            pass_on(passed + s)

        return carry

    lax.fori_loop(0, seqs, behind, 0)

    corr = []
    for q in range(SPAN // 16):
        corr += [corr_re[8 * q : 8 * q + 8, :], corr_im[8 * q : 8 * q + 8, :]]
    corr_high, corr_low = split(jnp.concatenate(corr, axis=0))
    taps_grad = dot(table[TAPI : TAPI + 64], corr_high)
    taps_grad = taps_grad[:32] + taps_grad[32:] + dot(table[TAPI : TAPI + 32], corr_low)
    small[:32, :] = taps_grad
    small[32:33, :] = jnp.sum(bias_acc[...], axis=0, keepdims=True)
    small[33:34, :] = jnp.sum(gain_acc[...], axis=0, keepdims=True)
    small[34:, :] = jnp.zeros((small.shape[0] - 34, chans), F32)
    small_copies = [
        remote(small, small_in.at[d - 1], small_send.at[d - 1], small_recv.at[d - 1], "sp", d)
        for d in sp_peers
    ]
    for copy in small_copies:
        copy.start()

    for c in range(min(passed + seqs, parts), parts):
        pass_on(c)

    keep_head = jnp.where(me < sp_devices - 1, 1.0, 0.0).astype(F32)
    for s in range(seqs):
        head_copy(s).wait()
        heads_ref[s] = heads_in[s] * keep_head
    total = small[...]
    for d, copy in zip(sp_peers, small_copies):
        copy.wait()
        total = total + small_in[d - 1]
    small_ref[...] = total
    for c in range(parts):
        columns = slice(c * part_width, (c + 1) * part_width)
        result = weight_grad[inner, outer, :, columns].astype(F32)
        result = result + pair[outer, :, columns].astype(F32)
        for d in range(1, groups):
            onward_copy(d, c).wait()
            result = result + arrived[d - 1, :, columns].astype(F32)
        weight_out_ref[:, columns] = result
    for s in range(seqs):
        spread_copy(s).wait()


def finish_kernel(
    seq_blocks, spread_ref, heads_ref, values_ref, gates_ref, small_ref, weight_ref,
    values_grad_ref, gates_grad_ref, taps_grad_ref, gain_grad_ref, bias_grad_ref, weight_grad_ref,
    gated_grad,
):
    step = pl.program_id(0)
    rows = spread_ref.shape[0]
    share = jnp.where(lax.rem(step, seq_blocks) == seq_blocks - 1, 1.0, 0.0).astype(F32)

    @pl.when(step == 0)
    def _():
        taps_grad_ref[...] = small_ref[:K]
        bias_grad_ref[...] = small_ref[32:33]
        gain_grad_ref[...] = small_ref[33:34]
        weight_grad_ref[...] = weight_ref[...]

    gated_grad[...] = spread_ref[...]
    gated_grad[rows - HALO :, :] += heads_ref[...] * share
    for i in range(rows // LANES):
        here = slice(i * LANES, (i + 1) * LANES)
        sig = sigmoid(gates_ref[here, :].astype(F32))
        values_part = gated_grad[here, :] * sig
        values_grad_ref[here, :] = values_part.astype(BF16)
        gates_part = values_part * values_ref[here, :].astype(F32) * (1.0 - sig)
        gates_grad_ref[here, :] = gates_part.astype(BF16)


def whole(shape):
    return pl.BlockSpec(shape, lambda i: (0,) * len(shape))


def on_device(values_in, gates_in, conv_taps, conv_bias, norm_gain, out_weight, out_grad):
    seqs, tokens, chans = values_in.shape
    width = out_grad.shape[2]
    total_chans = chans * lax.axis_size("tp")
    positions = seqs * tokens
    rows = min(512, tokens)
    blocks = positions // rows
    seq_blocks = tokens // rows
    chunks = tokens // LANES
    windows = -(-tokens // STEP)
    parts = 8
    tp_others = lax.axis_size("tp") - 1
    sp_devices = lax.axis_size("sp")
    sp_others = sp_devices - 1
    groups = sp_devices // PAIR
    weight_rows = chans // sp_devices
    small_rows = 40

    def dma(*shape):
        return pltpu.SemaphoreType.DMA(shape)

    anywhere = pl.BlockSpec(memory_space=pl.ANY)
    vmem = pl.BlockSpec(memory_space=pltpu.VMEM)
    padded = windows * STEP + HALO
    block_sums = (2, rows // LANES, LANES)
    spread, heads, small, weight_sum = pl.pallas_call(
        functools.partial(fused_kernel, total_chans),
        in_specs=[anywhere] * 5 + [vmem] * 3,
        out_specs=[anywhere] + [vmem] * 3,
        out_shape=[
            jax.ShapeDtypeStruct((seqs, tokens, chans), F32),
            jax.ShapeDtypeStruct((seqs, HALO, chans), F32),
            jax.ShapeDtypeStruct((small_rows, chans), F32),
            jax.ShapeDtypeStruct((weight_rows, width), F32),
        ],
        scratch_shapes=[
            pltpu.VMEM((seqs, tokens, chans), BF16),
            pltpu.VMEM((seqs, tokens, chans), BF16),
            pltpu.VMEM((seqs, HALO, chans), BF16),
            pltpu.VMEM((seqs, HALO, chans), BF16),
            pltpu.VMEM((positions, width), BF16),
            pltpu.VMEM((chans, max(positions, width)), BF16),
            pltpu.VMEM((width, chans), BF16),
            pltpu.VMEM((PAIR, groups, weight_rows, width), BF16),
            pltpu.VMEM((groups, weight_rows, width), BF16),
            pltpu.VMEM((groups - 1, weight_rows, width), BF16),
            pltpu.VMEM((groups - 1, weight_rows, width), BF16),
            pltpu.VMEM((seqs, tokens, chans), F32),
            pltpu.VMEM((2, rows, chans), F32),
            pltpu.VMEM((padded, chans), BF16),
            pltpu.VMEM((seqs * windows, SPAN, chans), BF16),
            pltpu.VMEM((windows, SPAN, chans), BF16),
            pltpu.VMEM((windows, SPAN, chans), BF16),
            pltpu.VMEM((padded, chans), BF16),
            pltpu.VMEM((padded, chans), BF16),
            pltpu.VMEM((TABLE_ROWS, SPAN), BF16),
            pltpu.VMEM((SPAN, chans), F32),
            pltpu.VMEM((SPAN // 2, chans), F32),
            pltpu.VMEM((SPAN // 2, chans), F32),
            pltpu.VMEM((SPAN // 2, chans), F32),
            pltpu.VMEM((SPAN // 2, chans), F32),
            pltpu.VMEM((seqs, HALO, chans), F32),
            pltpu.VMEM((seqs, HALO, chans), F32),
            pltpu.VMEM((seqs, 2, chunks, LANES), F32),
            pltpu.VMEM((tp_others, seqs, 2, chunks, LANES), F32),
            pltpu.VMEM((seqs, chunks, LANES), F32),
            pltpu.VMEM((blocks, *block_sums), F32),
            pltpu.VMEM((tp_others, blocks, *block_sums), F32),
            pltpu.VMEM((8, chans), F32),
            pltpu.VMEM((8, chans), F32),
            pltpu.VMEM((small_rows, chans), F32),
            pltpu.VMEM((sp_others, small_rows, chans), F32),
            dma(2, seqs),
            dma(blocks),
            dma(2),
            dma(seqs),
            dma(2),
            dma(2),
            dma(tp_others, seqs),
            dma(tp_others, seqs),
            dma(tp_others, blocks),
            dma(tp_others, blocks),
            dma(parts),
            dma(parts),
            dma(groups - 1, parts),
            dma(groups - 1, parts),
            dma(seqs),
            dma(seqs),
            dma(sp_others),
            dma(sp_others),
        ],
        compiler_params=pltpu.CompilerParams(
            vmem_limit_bytes=VMEM_LIMIT, collective_id=0, has_side_effects=True
        ),
        name="fused",
    )(
        values_in, gates_in, out_grad.reshape(positions, width), out_weight,
        jnp.asarray(transform_table()), conv_taps, conv_bias, norm_gain,
    )

    tile = pl.BlockSpec((rows, chans), lambda i: (i, 0))
    values_grad, gates_grad, taps_grad, gain_grad, bias_grad, weight_grad = pl.pallas_call(
        functools.partial(finish_kernel, seq_blocks),
        grid=(blocks,),
        in_specs=[
            tile, pl.BlockSpec((HALO, chans), lambda i: (i // seq_blocks, 0)), tile, tile,
            whole((small_rows, chans)), whole((weight_rows, width)),
        ],
        out_specs=[
            tile, tile, whole((K, chans)), whole((1, chans)), whole((1, chans)),
            whole((weight_rows, width)),
        ],
        out_shape=[
            jax.ShapeDtypeStruct((positions, chans), BF16),
            jax.ShapeDtypeStruct((positions, chans), BF16),
            jax.ShapeDtypeStruct((K, chans), F32),
            jax.ShapeDtypeStruct((1, chans), F32),
            jax.ShapeDtypeStruct((1, chans), F32),
            jax.ShapeDtypeStruct((weight_rows, width), F32),
        ],
        scratch_shapes=[pltpu.VMEM((rows, chans), F32)],
        compiler_params=pltpu.CompilerParams(dimension_semantics=("arbitrary",)),
        name="finish",
    )(
        spread.reshape(positions, chans), heads.reshape(seqs * HALO, chans),
        values_in.reshape(positions, chans), gates_in.reshape(positions, chans),
        small, weight_sum,
    )
    return (
        values_grad.reshape(values_in.shape),
        gates_grad.reshape(values_in.shape),
        taps_grad,
        gain_grad[0],
        bias_grad[0],
        weight_grad,
    )


def solution(mesh):
    return jax.shard_map(
        on_device,
        mesh=mesh,
        in_specs=(
            P(None, "sp", "tp"),
            P(None, "sp", "tp"),
            P(None, "tp"),
            P("tp"),
            P("tp"),
            P("tp", None),
            P(None, "sp", None),
        ),
        out_specs=(
            P(None, "sp", "tp"),
            P(None, "sp", "tp"),
            P(None, "tp"),
            P("tp"),
            P("tp"),
            P(("tp", "sp"), None),
        ),
        check_vma=False,
    )
```

```python
import functools

import jax
import jax.numpy as jnp
import numpy as np
from jax import lax
from jax.experimental import pallas as pl
from jax.experimental.pallas import tpu as pltpu
from jax.sharding import PartitionSpec as P

K = 31
EPS = 1e-05
HALO = 32
PAIR = 2
LANES = 128
SPAN = 256
STEP = SPAN - HALO
F32 = jnp.float32
BF16 = jnp.bfloat16
VMEM_LIMIT = 64 * 1024 * 1024 - 64 * 1024

FWD, GRAD, INV, CONV, TAPF, TAPI = 0, 512, 1024, 1536, 1984, 2496
TABLE_ROWS = 2560


def transform_table():
    row = np.arange(SPAN)
    freq = 8 * (row // 16) + row % 8
    angle = 2 * np.pi * (freq[:, None] + 0.5) * np.arange(SPAN)[None] / SPAN
    fwd = np.where((row // 8 % 2 == 0)[:, None], np.cos(angle), -np.sin(angle))
    inv = fwd.T * (2 / SPAN)
    grad = np.zeros((SPAN, SPAN))
    grad[:, :STEP] = fwd[:, HALO:]
    tap_fwd = np.zeros((SPAN, SPAN))
    tap_fwd[:, :K] = fwd[:, K - 1 :: -1]
    tap_inv = np.zeros((32, SPAN))
    tap_inv[:K] = inv[K - 1 :: -1]
    parts = []
    for whole_part in (fwd, grad, inv, inv[HALO:], tap_fwd, tap_inv):
        high = whole_part.astype(BF16)
        parts += [high, (whole_part - high.astype(np.float64)).astype(BF16)]
    return np.concatenate(parts)


def sigmoid(x):
    return 0.5 * jnp.tanh(0.5 * x) + 0.5


def peer_id(axis, distance):
    devices = lax.axis_size(axis)
    return {axis: lax.rem(lax.axis_index(axis) + distance, devices)}


def greet(pairs):
    barrier = pltpu.get_barrier_semaphore()
    for axis, distance in pairs:
        pl.semaphore_signal(
            barrier, inc=1, device_id=peer_id(axis, distance),
            device_id_type=pl.DeviceIdType.MESH,
        )
    pl.semaphore_wait(barrier, len(pairs))


def remote(src, dst, send_sem, recv_sem, axis, distance):
    return pltpu.make_async_remote_copy(
        src_ref=src, dst_ref=dst, send_sem=send_sem, recv_sem=recv_sem,
        device_id=peer_id(axis, distance), device_id_type=pl.DeviceIdType.MESH,
    )


def dot(a, b):
    return jnp.dot(a, b, preferred_element_type=F32)


def lane_sums(x):
    return jnp.sum(x.T, axis=0, keepdims=True)


def row_spread(row):
    return jnp.broadcast_to(row, (LANES, LANES)).T


def split(x):
    high = x.astype(BF16)
    return high, (x - high.astype(F32)).astype(BF16)


def fused_kernel(
    total_chans, values_hbm, gates_hbm, cot_hbm, weight_hbm, table_hbm, taps_hbm, bias_hbm,
    gain_hbm,
    spread_hbm, heads_hbm, small_hbm, weight_out_hbm,
    values, gates, values_halo, gates_halo, cot, swished, weight, weight_t, weight_grad, pair,
    onward, arrived, weight_sum, conv, grad, x_first, x_last, spectrum, high, low, grad_high, grad_low, table,
    taps, bias_row, gain_row, tap_rows,
    tap_re, tap_im, corr_re, corr_im, heads, heads_in, sums, sums_in, stat, back, back_in,
    gain_acc, bias_acc, small, small_sum, small_in,
    load_sems, cot_sems, misc_sems, out_sems, weight_sems, halo_send, halo_recv, sums_send, sums_recv,
    back_send, back_recv, pair_send, pair_recv, onward_send, onward_recv, head_send, head_recv,
    small_send, small_recv,
):
    seqs, tokens, chans = values.shape
    positions, width = cot.shape
    lane_blocks = chans // LANES
    chunks = tokens // LANES
    windows = spectrum.shape[0] // seqs
    rows = grad.shape[1]
    blocks = positions // rows
    strips = cot_sems.shape[0]
    strip_width = width // strips
    seq_blocks = blocks // seqs
    block_chunks = rows // LANES
    parts = pair_send.shape[0]
    part_width = width // parts
    groups, weight_rows = pair.shape[0], pair.shape[1]
    sp_devices = lax.axis_size("sp")
    me = lax.axis_index("sp")
    inner = lax.rem(me, PAIR)
    outer = me // PAIR
    tp_peers = range(1, lax.axis_size("tp"))
    sp_peers = range(1, sp_devices)

    def seq_loads(s):
        return [
            pltpu.make_async_copy(src.at[s], dst.at[s], load_sems.at[n, s])
            for n, (src, dst) in enumerate(((values_hbm, values), (gates_hbm, gates)))
        ]

    table_load = pltpu.make_async_copy(table_hbm, table, misc_sems.at[0])
    row_loads = [
        pltpu.make_async_copy(src, dst, misc_sems.at[n])
        for n, (src, dst) in enumerate(
            ((taps_hbm, taps), (bias_hbm, bias_row), (gain_hbm, gain_row)), 2
        )
    ]
    weight_load = pltpu.make_async_copy(weight_hbm, weight, misc_sems.at[1])

    def strip(i):
        return pl.ds(pl.multiple_of(i * strip_width, strip_width), strip_width)

    def cot_load(i):
        return pltpu.make_async_copy(cot_hbm.at[:, strip(i)], cot.at[:, strip(i)], cot_sems.at[i])

    for copy in row_loads:
        copy.start()
    for copy in seq_loads(0):
        copy.start()
    table_load.start()
    for s in range(1, seqs):
        for copy in seq_loads(s):
            copy.start()
    weight_load.start()

    greet([("tp", d) for d in tp_peers] + [("sp", d) for d in sp_peers])
    last = pl.ds(tokens - HALO, HALO)
    halo_copies = [
        remote(src.at[:, last], dst, halo_send.at[n], halo_recv.at[n], "sp", 1)
        for n, (src, dst) in enumerate(((values_hbm, values_halo), (gates_hbm, gates_halo)))
    ]
    for copy in halo_copies:
        copy.start()

    tail = tokens - (windows - 1) * STEP + HALO
    x_last[tail:, :] = jnp.zeros((SPAN - tail, chans), BF16)
    for ref in (grad_high, grad_low):
        ref[tokens:, :] = jnp.zeros((ref.shape[0] - tokens, chans), BF16)
    for ref in (gain_acc, bias_acc, corr_re, corr_im, tap_rows):
        ref[...] = jnp.zeros_like(ref)
    for copy in row_loads:
        copy.wait()
    tap_rows[:K, :] = taps[...].astype(F32)
    bias = bias_row[...].astype(F32).reshape(1, chans)
    gain = gain_row[...].astype(F32).reshape(1, chans)

    table_load.wait()
    taps_wide = dot(table[TAPF : TAPF + 2 * SPAN], tap_rows[...].astype(BF16))
    taps_wide = taps_wide[:SPAN] + taps_wide[SPAN:]
    for q in range(SPAN // 16):
        tap_re[8 * q : 8 * q + 8, :] = taps_wide[16 * q : 16 * q + 8]
        tap_im[8 * q : 8 * q + 8, :] = taps_wide[16 * q + 8 : 16 * q + 16]

    def gate(values_part, gates_part):
        return (values_part.astype(F32) * sigmoid(gates_part.astype(F32))).astype(BF16)

    def gate_all(s, carry):
        for copy in seq_loads(s):
            copy.wait()
        for i in range(chunks):
            here = slice(i * LANES, (i + 1) * LANES)
            gated = gate(values[s, here, :], gates[s, here, :])
            values[s, here, :] = gated
            count = min(STEP - i * LANES, LANES)
            if count > 0:
                x_first[s, HALO + i * LANES : HALO + i * LANES + count, :] = gated[:count]
        return carry

    lax.fori_loop(0, seqs, gate_all, 0)
    for i in range(strips):
        cot_load(i).start()

    def turn(i, carry):
        here = pl.ds(pl.multiple_of(i * 512, 512), 512)
        weight_t[here, :] = weight[:, here].T
        return carry

    def product(x, sign, high_ref, low_ref):
        for q in range(SPAN // 16):
            a, b = tap_re[8 * q : 8 * q + 8, :], tap_im[8 * q : 8 * q + 8, :]
            re, im = x[16 * q : 16 * q + 8], x[16 * q + 8 : 16 * q + 16]
            if sign > 0:
                both = (a * re - b * im, a * im + b * re)
            else:
                both = (a * re + b * im, a * im - b * re)
            here = slice(16 * q, 16 * q + 16)
            high_ref[here, :], low_ref[here, :] = split(jnp.concatenate(both, axis=0))

    def sums_copies(s):
        return [
            remote(sums.at[s], sums_in.at[d - 1, s], sums_send.at[d - 1, s],
                   sums_recv.at[d - 1, s], "tp", d)
            for d in tp_peers
        ]

    weight_load.wait()
    lax.fori_loop(0, width // 512, turn, 0)
    for copy in halo_copies:
        copy.wait()
    keep = jnp.where(me > 0, 1.0, 0.0).astype(F32)
    for s in range(seqs):
        x_first[s, :HALO, :] = gate(values_halo[s].astype(F32) * keep, gates_halo[s])

    def ahead(s, carry):
        x_last[:tail, :] = values[s, tokens - tail :, :]
        for w in range(windows):
            if w == 0:
                x = x_first[s]
            elif w < windows - 1:
                x = values[s, w * STEP - HALO : w * STEP + STEP, :]
            else:
                x = x_last[...]
            x = dot(table[FWD : FWD + 2 * SPAN], x)
            x = x[:SPAN] + x[SPAN:]
            spectrum[s * windows + w] = x.astype(BF16)
            product(x, 1, high.at[w], low.at[w])
        for w in range(windows):
            y = dot(table[CONV : CONV + 2 * STEP], high[w])
            y = y[:STEP] + y[STEP:] + dot(table[CONV : CONV + STEP], low[w]) + bias
            count = min(STEP, tokens - w * STEP)
            conv[s, w * STEP : w * STEP + count, :] = y[:count]
        for i in range(chunks):
            total = square = None
            for h in range(lane_blocks):
                part = conv[s, i * LANES : (i + 1) * LANES, h * LANES : (h + 1) * LANES]
                total = part if total is None else total + part
                square = part * part if square is None else square + part * part
            sums[s, 0, i : i + 1, :] = lane_sums(total)
            sums[s, 1, i : i + 1, :] = lane_sums(square)
        for copy in sums_copies(s):
            copy.start()
        return carry

    lax.fori_loop(0, seqs, ahead, 0)

    def norm(s, carry):
        total = sums[s]
        for d, copy in zip(tp_peers, sums_copies(s)):
            copy.wait()
            total = total + sums_in[d - 1, s]
        mean_rows = total[0] / total_chans
        variance = total[1] / total_chans - mean_rows * mean_rows
        inverse_rows = lax.rsqrt(variance + EPS)
        stat[s] = inverse_rows
        for i in range(chunks):
            here = slice(i * LANES, (i + 1) * LANES)
            columns = pl.ds(pl.multiple_of(s * tokens + i * LANES, LANES), LANES)
            mean = row_spread(mean_rows[i : i + 1])
            inverse = row_spread(inverse_rows[i : i + 1])
            for h in range(lane_blocks):
                lanes = slice(h * LANES, (h + 1) * LANES)
                normed = (conv[s, here, lanes] - mean) * inverse
                conv[s, here, lanes] = normed
                scaled = normed * gain[:, lanes]
                swished[lanes, columns] = (scaled * sigmoid(scaled)).astype(BF16).T
        return carry

    lax.fori_loop(0, seqs, norm, 0)

    def part_columns(c):
        return pl.ds(pl.multiple_of(c * part_width, part_width), part_width)

    def pair_copy(c):
        columns = part_columns(c)
        return remote(
            weight_grad.at[1 - inner, :, :, columns], pair.at[:, :, columns], pair_send.at[c],
            pair_recv.at[c], "sp", sp_devices + 1 - 2 * inner,
        )

    def onward_copy(d, c):
        columns = part_columns(c)
        return remote(
            onward.at[d - 1, :, columns], arrived.at[d - 1, :, columns], onward_send.at[d - 1, c],
            onward_recv.at[d - 1, c], "sp", d * PAIR,
        )

    def pass_on(c):
        columns = part_columns(c)
        pair_copy(c).wait()
        for d in range(1, groups):
            target = lax.rem(outer + d, groups)
            onward[d - 1, :, columns] = (
                weight_grad[inner, target, :, columns].astype(F32)
                + pair[target, :, columns].astype(F32)
            ).astype(BF16)
        for d in range(1, groups):
            onward_copy(d, c).start()

    def project(i, carry):
        cot_load(i).wait()
        result = dot(swished[...], cot[:, strip(i)])
        for g in range(groups):
            for n in range(PAIR):
                first = (g * PAIR + n) * weight_rows
                weight_grad[n, g, :, strip(i)] = result[first : first + weight_rows].astype(BF16)
        for n in range(strip_parts):
            pair_copy(i * strip_parts + n).start()

        @pl.when(i >= lag)
        def _():
            pass_on(i - lag)

        return carry

    lag = min(3, strips)
    strip_parts = parts // strips
    lax.fori_loop(0, strips, project, 0)
    passed = strips - lag

    def back_copies(j):
        return [
            remote(back.at[j], back_in.at[d - 1, j], back_send.at[d - 1, j],
                   back_recv.at[d - 1, j], "tp", d)
            for d in tp_peers
        ]

    def multiply(j):
        here = pl.ds(pl.multiple_of(j * rows, rows), rows)
        grad[lax.rem(j, 2)] = dot(cot[here, :], weight_t[...])

    def middle(j):
        s = j // seq_blocks
        first = lax.rem(j, seq_blocks) * rows
        slot = lax.rem(j, 2)
        for i in range(block_chunks):
            here = pl.ds(pl.multiple_of(first + i * LANES, LANES), LANES)
            plain = weighted = None
            for h in range(lane_blocks):
                lanes = slice(h * LANES, (h + 1) * LANES)
                normed = conv[s, here, lanes]
                scaled = normed * gain[:, lanes]
                sig = sigmoid(scaled)
                silu = scaled * sig
                scaled_grad = grad[slot, i * LANES : (i + 1) * LANES, lanes] * (
                    sig + silu * (1.0 - sig)
                )
                normed_grad = scaled_grad * gain[:, lanes]
                values[s, here, lanes], gates[s, here, lanes] = split(normed_grad)
                term = scaled_grad * normed
                gain_acc[:, lanes] += jnp.sum(term.reshape(LANES // 8, 8, LANES), axis=0)
                term = normed_grad * normed
                plain = normed_grad if plain is None else plain + normed_grad
                weighted = term if weighted is None else weighted + term
            back[j, 0, i : i + 1, :] = lane_sums(plain)
            back[j, 1, i : i + 1, :] = lane_sums(weighted)
        for copy in back_copies(j):
            copy.start()

    multiply(0)

    def both(j, carry):
        middle(j - 1)
        multiply(j)

        @pl.when(passed + j - 1 < parts)
        def _():
            pass_on(passed + j - 1)

        return carry

    lax.fori_loop(1, blocks, both, 0)
    middle(blocks - 1)
    passed_on = passed + blocks - 1
    if passed_on < parts:
        pass_on(passed_on)
        passed_on += 1

    def spread_copy(s):
        return pltpu.make_async_copy(conv.at[s], spread_hbm.at[s], out_sems.at[s])

    def head_copy(s):
        return remote(
            heads.at[s], heads_in.at[s], head_send.at[s], head_recv.at[s], "sp", sp_devices - 1
        )

    per = tokens // SPAN

    def spread_parts(s, w):
        here = pl.ds(pl.multiple_of(s * tokens + w % per * SPAN, SPAN), SPAN)
        return spectrum.at[s * windows + w], cot.at[here, pl.ds(w // per * chans, chans)]

    def behind(s, carry):
        for n in range(seq_blocks):
            for copy in back_copies(s * seq_blocks + n):
                copy.wait()
        for i in range(chunks):
            here = slice(i * LANES, (i + 1) * LANES)
            j = s * seq_blocks + i // block_chunks
            at = slice(i % block_chunks, i % block_chunks + 1)
            inverse_row = stat[s, i : i + 1, :]
            plain, weighted = back[j, 0, at, :], back[j, 1, at, :]
            for d in tp_peers:
                plain = plain + back_in[d - 1, j, 0, at, :]
                weighted = weighted + back_in[d - 1, j, 1, at, :]
            scale = inverse_row / total_chans
            inverse = row_spread(inverse_row)
            plain = row_spread(plain * scale)
            weighted = row_spread(weighted * scale)
            for h in range(lane_blocks):
                lanes = slice(h * LANES, (h + 1) * LANES)
                normed_grad = values[s, here, lanes].astype(F32) + gates[s, here, lanes].astype(
                    F32
                )
                conv_grad = inverse * normed_grad - plain - conv[s, here, lanes] * weighted
                grad_high[here, lanes], grad_low[here, lanes] = split(conv_grad)
                bias_acc[:, lanes] += jnp.sum(conv_grad.reshape(LANES // 8, 8, LANES), axis=0)
        for w in range(windows):
            here = slice(w * STEP, w * STEP + SPAN)
            g = dot(table[GRAD : GRAD + 2 * SPAN], grad_high[here, :])
            g = g[:SPAN] + g[SPAN:] + dot(table[GRAD : GRAD + SPAN], grad_low[here, :])
            x = spectrum[s * windows + w].astype(F32)
            for q in range(SPAN // 16):
                at = slice(8 * q, 8 * q + 8)
                g_re, g_im = g[16 * q : 16 * q + 8], g[16 * q + 8 : 16 * q + 16]
                x_re, x_im = x[16 * q : 16 * q + 8], x[16 * q + 8 : 16 * q + 16]
                corr_re[at, :] += g_re * x_re + g_im * x_im
                corr_im[at, :] += g_im * x_re - g_re * x_im
            product(g, -1, *spread_parts(s, w))

        @pl.when(passed_on + s < parts)
        def _():
            pass_on(passed_on + s)

        return carry

    lax.fori_loop(0, seqs, behind, 0)

    corr = []
    for q in range(SPAN // 16):
        corr += [corr_re[8 * q : 8 * q + 8, :], corr_im[8 * q : 8 * q + 8, :]]
    corr_high, corr_low = split(jnp.concatenate(corr, axis=0))
    taps_grad = dot(table[TAPI : TAPI + 64], corr_high)
    taps_grad = taps_grad[:32] + taps_grad[32:] + dot(table[TAPI : TAPI + 32], corr_low)
    small[:32, :] = taps_grad
    small[32:33, :] = jnp.sum(bias_acc[...], axis=0, keepdims=True)
    small[33:34, :] = jnp.sum(gain_acc[...], axis=0, keepdims=True)
    small[34:, :] = jnp.zeros((small.shape[0] - 34, chans), F32)
    small_pair = remote(
        small, small_in.at[0], small_send.at[0], small_recv.at[0], "sp",
        sp_devices + 1 - 2 * inner,
    )
    small_pair.start()
    for c in range(min(passed_on + seqs, parts), parts):
        pass_on(c)

    def spread_window(s, w):
        high_ref, low_ref = spread_parts(s, w)
        y = dot(table[INV : INV + 2 * SPAN], high_ref[...])
        y = y[:SPAN] + y[SPAN:] + dot(table[INV : INV + SPAN], low_ref[...])
        count = min(STEP, tokens - w * STEP)
        conv[s, w * STEP : w * STEP + count, :] = y[HALO : HALO + count]
        return y[:HALO]

    for s in range(seqs):
        heads[s] = spread_window(s, 0)
    for s in range(seqs):
        head_copy(s).start()
    small_pair.wait()
    small_sum[...] = small[...] + small_in[0]
    small_copies = [
        remote(small_sum, small_in.at[d], small_send.at[d], small_recv.at[d], "sp", d * PAIR)
        for d in range(1, groups)
    ]
    for copy in small_copies:
        copy.start()

    def spread_rest(s, carry):
        for w in range(1, windows):
            conv[s, w * STEP - HALO : w * STEP, :] += spread_window(s, w)
        spread_copy(s).start()
        return carry

    lax.fori_loop(0, seqs, spread_rest, 0)

    outs = []
    for c in range(parts):
        columns = slice(c * part_width, (c + 1) * part_width)
        result = weight_grad[inner, outer, :, columns].astype(F32)
        result = result + pair[outer, :, columns].astype(F32)
        for d in range(1, groups):
            onward_copy(d, c).wait()
            result = result + arrived[d - 1, :, columns].astype(F32)
        weight_sum[:, columns] = result
        if (c + 1) % strip_parts == 0:
            columns = pl.ds(c // strip_parts * strip_width, strip_width)
            outs.append(pltpu.make_async_copy(
                weight_sum.at[:, columns], weight_out_hbm.at[:, columns],
                weight_sems.at[c // strip_parts],
            ))
            outs[-1].start()
    keep_head = jnp.where(me < sp_devices - 1, 1.0, 0.0).astype(F32)
    for s in range(seqs):
        head_copy(s).wait()
        heads_in[s] = heads_in[s] * keep_head
    outs.append(pltpu.make_async_copy(heads_in, heads_hbm, misc_sems.at[0]))
    outs[-1].start()
    total = small_sum[...]
    for d, copy in enumerate(small_copies, 1):
        copy.wait()
        total = total + small_in[d]
    small[...] = total
    outs.append(pltpu.make_async_copy(small, small_hbm, misc_sems.at[1]))
    outs[-1].start()
    for copy in outs:
        copy.wait()
    for s in range(seqs):
        spread_copy(s).wait()


def finish_kernel(
    spread_hbm, values_hbm, gates_hbm, weight_hbm, heads_hbm, small_hbm,
    values_grad_hbm, gates_grad_hbm, weight_grad_hbm, taps_grad_hbm, gain_grad_hbm, bias_grad_hbm,
    spread, values, gates, weight, heads, small, taps_grad, gain_grad, bias_grad,
    load_sems, out_sems, in_sems, end_sems,
):
    seqs, tokens, chans = spread.shape
    seq_blocks = load_sems.shape[1] // seqs
    rows = tokens // seq_blocks
    loads, stores = [], []
    extra = [
        pltpu.make_async_copy(src, dst, in_sems.at[n])
        for n, (src, dst) in enumerate(
            ((heads_hbm, heads), (small_hbm, small), (weight_hbm, weight))
        )
    ]
    ends = [
        pltpu.make_async_copy(src, dst, end_sems.at[n])
        for n, (src, dst) in enumerate((
            (taps_grad, taps_grad_hbm), (gain_grad, gain_grad_hbm), (bias_grad, bias_grad_hbm),
            (weight, weight_grad_hbm),
        ))
    ]
    for copy in extra[:2]:
        copy.start()
    for n in range(seqs * seq_blocks):
        s, here = n // seq_blocks, pl.ds(n % seq_blocks * rows, rows)
        pairs = ((spread_hbm, spread), (values_hbm, values), (gates_hbm, gates))
        loads.append([
            pltpu.make_async_copy(src.at[s, here], dst.at[s, here], load_sems.at[m, n])
            for m, (src, dst) in enumerate(pairs)
        ])
        for copy in loads[n]:
            copy.start()
    extra[2].start()
    for copy in extra[:2]:
        copy.wait()
    taps_grad[...] = small[:K]
    bias_grad[...] = small[32:33]
    gain_grad[...] = small[33:34]
    for copy in ends[:3]:
        copy.start()
    for n in range(seqs * seq_blocks):
        s, first = n // seq_blocks, n % seq_blocks * rows
        for copy in loads[n]:
            copy.wait()
        if n % seq_blocks == seq_blocks - 1:
            spread[s, tokens - HALO :, :] += heads[s]
        for i in range(rows // LANES):
            here = slice(first + i * LANES, first + (i + 1) * LANES)
            sig = sigmoid(gates[s, here, :].astype(F32))
            values_part = spread[s, here, :] * sig
            gates_part = values_part * values[s, here, :].astype(F32) * (1.0 - sig)
            values[s, here, :] = values_part.astype(BF16)
            gates[s, here, :] = gates_part.astype(BF16)
        for m, (src, dst) in enumerate(((values, values_grad_hbm), (gates, gates_grad_hbm))):
            copy = pltpu.make_async_copy(
                src.at[s, pl.ds(first, rows)], dst.at[s, pl.ds(first, rows)], out_sems.at[m, n]
            )
            copy.start()
            stores.append(copy)
    extra[2].wait()
    ends[3].start()
    for copy in stores + ends:
        copy.wait()


def on_device(values_in, gates_in, conv_taps, conv_bias, norm_gain, out_weight, out_grad):
    seqs, tokens, chans = values_in.shape
    width = out_grad.shape[2]
    total_chans = chans * lax.axis_size("tp")
    positions = seqs * tokens
    rows = min(512, tokens)
    blocks = positions // rows
    chunks = tokens // LANES
    windows = -(-tokens // STEP)
    strips = 8
    parts = 16
    tp_others = lax.axis_size("tp") - 1
    sp_devices = lax.axis_size("sp")
    groups = sp_devices // PAIR
    weight_rows = chans // sp_devices
    small_rows = 40

    def dma(*shape):
        return pltpu.SemaphoreType.DMA(shape)

    anywhere = pl.BlockSpec(memory_space=pl.ANY)
    padded = windows * STEP + HALO
    block_sums = (2, rows // LANES, LANES)
    spread, heads, small, weight_sum = pl.pallas_call(
        functools.partial(fused_kernel, total_chans),
        in_specs=[anywhere] * 8,
        out_specs=[anywhere] * 4,
        out_shape=[
            jax.ShapeDtypeStruct((seqs, tokens, chans), F32),
            jax.ShapeDtypeStruct((seqs, HALO, chans), F32),
            jax.ShapeDtypeStruct((small_rows, chans), F32),
            jax.ShapeDtypeStruct((weight_rows, width), F32),
        ],
        scratch_shapes=[
            pltpu.VMEM((seqs, tokens, chans), BF16),
            pltpu.VMEM((seqs, tokens, chans), BF16),
            pltpu.VMEM((seqs, HALO, chans), BF16),
            pltpu.VMEM((seqs, HALO, chans), BF16),
            pltpu.VMEM((positions, width), BF16),
            pltpu.VMEM((chans, positions), BF16),
            pltpu.VMEM((chans, width), BF16),
            pltpu.VMEM((width, chans), BF16),
            pltpu.VMEM((PAIR, groups, weight_rows, width), BF16),
            pltpu.VMEM((groups, weight_rows, width), BF16),
            pltpu.VMEM((groups - 1, weight_rows, width), BF16),
            pltpu.VMEM((groups - 1, weight_rows, width), BF16),
            pltpu.VMEM((weight_rows, width), F32),
            pltpu.VMEM((seqs, tokens, chans), F32),
            pltpu.VMEM((2, rows, chans), F32),
            pltpu.VMEM((seqs, SPAN, chans), BF16),
            pltpu.VMEM((SPAN, chans), BF16),
            pltpu.VMEM((seqs * windows, SPAN, chans), BF16),
            pltpu.VMEM((windows, SPAN, chans), BF16),
            pltpu.VMEM((windows, SPAN, chans), BF16),
            pltpu.VMEM((padded, chans), BF16),
            pltpu.VMEM((padded, chans), BF16),
            pltpu.VMEM((TABLE_ROWS, SPAN), BF16),
            pltpu.VMEM((K, chans), BF16),
            pltpu.VMEM((chans,), BF16),
            pltpu.VMEM((chans,), BF16),
            pltpu.VMEM((SPAN, chans), F32),
            pltpu.VMEM((SPAN // 2, chans), F32),
            pltpu.VMEM((SPAN // 2, chans), F32),
            pltpu.VMEM((SPAN // 2, chans), F32),
            pltpu.VMEM((SPAN // 2, chans), F32),
            pltpu.VMEM((seqs, HALO, chans), F32),
            pltpu.VMEM((seqs, HALO, chans), F32),
            pltpu.VMEM((seqs, 2, chunks, LANES), F32),
            pltpu.VMEM((tp_others, seqs, 2, chunks, LANES), F32),
            pltpu.VMEM((seqs, chunks, LANES), F32),
            pltpu.VMEM((blocks, *block_sums), F32),
            pltpu.VMEM((tp_others, blocks, *block_sums), F32),
            pltpu.VMEM((8, chans), F32),
            pltpu.VMEM((8, chans), F32),
            pltpu.VMEM((small_rows, chans), F32),
            pltpu.VMEM((small_rows, chans), F32),
            pltpu.VMEM((groups, small_rows, chans), F32),
            dma(2, seqs),
            dma(strips),
            dma(5),
            dma(seqs),
            dma(strips),
            dma(2),
            dma(2),
            dma(tp_others, seqs),
            dma(tp_others, seqs),
            dma(tp_others, blocks),
            dma(tp_others, blocks),
            dma(parts),
            dma(parts),
            dma(groups - 1, parts),
            dma(groups - 1, parts),
            dma(seqs),
            dma(seqs),
            dma(groups),
            dma(groups),
        ],
        compiler_params=pltpu.CompilerParams(
            vmem_limit_bytes=VMEM_LIMIT, collective_id=0, has_side_effects=True
        ),
        name="fused",
    )(
        values_in, gates_in, out_grad.reshape(positions, width), out_weight,
        jnp.asarray(transform_table()), conv_taps, conv_bias, norm_gain,
    )

    values_grad, gates_grad, weight_grad, taps_grad, gain_grad, bias_grad = pl.pallas_call(
        finish_kernel,
        in_specs=[anywhere] * 6,
        out_specs=[anywhere] * 6,
        out_shape=[
            jax.ShapeDtypeStruct((seqs, tokens, chans), BF16),
            jax.ShapeDtypeStruct((seqs, tokens, chans), BF16),
            jax.ShapeDtypeStruct((weight_rows, width), F32),
            jax.ShapeDtypeStruct((K, chans), F32),
            jax.ShapeDtypeStruct((1, chans), F32),
            jax.ShapeDtypeStruct((1, chans), F32),
        ],
        scratch_shapes=[
            pltpu.VMEM((seqs, tokens, chans), F32),
            pltpu.VMEM((seqs, tokens, chans), BF16),
            pltpu.VMEM((seqs, tokens, chans), BF16),
            pltpu.VMEM((weight_rows, width), F32),
            pltpu.VMEM((seqs, HALO, chans), F32),
            pltpu.VMEM((small_rows, chans), F32),
            pltpu.VMEM((K, chans), F32),
            pltpu.VMEM((1, chans), F32),
            pltpu.VMEM((1, chans), F32),
            dma(3, blocks),
            dma(2, blocks),
            dma(3),
            dma(4),
        ],
        compiler_params=pltpu.CompilerParams(vmem_limit_bytes=VMEM_LIMIT),
        name="finish",
    )(spread, values_in, gates_in, weight_sum, heads, small)
    return values_grad, gates_grad, taps_grad, gain_grad[0], bias_grad[0], weight_grad


def solution(mesh):
    return jax.shard_map(
        on_device,
        mesh=mesh,
        in_specs=(
            P(None, "sp", "tp"),
            P(None, "sp", "tp"),
            P(None, "tp"),
            P("tp"),
            P("tp"),
            P("tp", None),
            P(None, "sp", None),
        ),
        out_specs=(
            P(None, "sp", "tp"),
            P(None, "sp", "tp"),
            P(None, "tp"),
            P("tp"),
            P("tp"),
            P(("tp", "sp"), None),
        ),
        check_vma=False,
    )
```

```python
import functools

import jax
import jax.numpy as jnp
import numpy as np
from jax import lax
from jax.experimental import pallas as pl
from jax.experimental.pallas import tpu as pltpu
from jax.sharding import PartitionSpec as P

K = 31
EPS = 1e-05
HALO = 32
PAIR = 2
LANES = 128
SPAN = 256
STEP = SPAN - HALO
F32 = jnp.float32
BF16 = jnp.bfloat16
VMEM_LIMIT = 64 * 1024 * 1024 - 64 * 1024

FWD, GRAD, INV, CONV, TAPF, TAPI = 0, 512, 1024, 1536, 1984, 2496
TABLE_ROWS = 2560


def transform_table():
    row = np.arange(SPAN)
    freq = 8 * (row // 16) + row % 8
    angle = 2 * np.pi * (freq[:, None] + 0.5) * np.arange(SPAN)[None] / SPAN
    fwd = np.where((row // 8 % 2 == 0)[:, None], np.cos(angle), -np.sin(angle))
    inv = fwd.T * (2 / SPAN)
    grad = np.zeros((SPAN, SPAN))
    grad[:, :STEP] = fwd[:, HALO:]
    tap_fwd = np.zeros((SPAN, SPAN))
    tap_fwd[:, :K] = fwd[:, K - 1 :: -1]
    tap_inv = np.zeros((32, SPAN))
    tap_inv[:K] = inv[K - 1 :: -1]
    parts = []
    for whole_part in (fwd, grad, inv, inv[HALO:], tap_fwd, tap_inv):
        high = whole_part.astype(BF16)
        parts += [high, (whole_part - high.astype(np.float64)).astype(BF16)]
    return np.concatenate(parts)


def sigmoid(x):
    return 0.5 * jnp.tanh(0.5 * x) + 0.5


def peer_id(axis, distance):
    devices = lax.axis_size(axis)
    return {axis: lax.rem(lax.axis_index(axis) + distance, devices)}


def greet(pairs):
    barrier = pltpu.get_barrier_semaphore()
    for axis, distance in pairs:
        pl.semaphore_signal(
            barrier, inc=1, device_id=peer_id(axis, distance),
            device_id_type=pl.DeviceIdType.MESH,
        )
    pl.semaphore_wait(barrier, len(pairs))


def remote(src, dst, send_sem, recv_sem, axis, distance):
    return pltpu.make_async_remote_copy(
        src_ref=src, dst_ref=dst, send_sem=send_sem, recv_sem=recv_sem,
        device_id=peer_id(axis, distance), device_id_type=pl.DeviceIdType.MESH,
    )


def arrive(ref, sem, axis):
    remote(ref, ref, sem, sem, axis, 1).wait_recv()


def dot(a, b):
    return jnp.dot(a, b, preferred_element_type=F32)


def lane_sums(x):
    return jnp.sum(x.T, axis=0, keepdims=True)


def row_spread(row):
    return jnp.broadcast_to(row, (LANES, LANES)).T


def split(x):
    high = x.astype(BF16)
    return high, (x - high.astype(F32)).astype(BF16)


def fused_kernel(
    total_chans, values_hbm, gates_hbm, cot_hbm, weight_hbm, table_hbm, taps_hbm, bias_hbm,
    gain_hbm,
    values_grad_hbm, gates_grad_hbm, small_hbm, weight_out_hbm,
    values, gates, values_halo, gates_halo, cot, swished, weight_t, weight_grad, pair,
    onward, arrived, weight_sum, conv, norm_grad, grad, x_first, x_last, spectrum, high, low, grad_high, grad_low, table,
    taps, bias_row, gain_row, tap_rows,
    tap_re, tap_im, corr_re, corr_im, heads, heads_in, sums, sums_in, stat, back, back_in,
    gain_acc, bias_acc, small, small_sum, small_total, small_in,
    load_sems, cot_sems, misc_sems, halo_send, halo_recv, sums_send, sums_recv,
    back_send, back_recv, pair_send, pair_recv, onward_send, onward_recv, head_send, head_recv,
    small_send, small_recv,
):
    seqs, tokens, chans = values.shape
    positions, width = cot.shape
    lane_blocks = chans // LANES
    chunks = tokens // LANES
    windows = spectrum.shape[0] // seqs
    rows = grad.shape[1]
    blocks = positions // rows
    strips = cot_sems.shape[0]
    strip_width = width // strips
    seq_blocks = blocks // seqs
    block_chunks = rows // LANES
    parts = pair_recv.shape[0]
    part_width = width // parts
    groups, weight_rows = pair.shape[0], pair.shape[1]
    sp_devices = lax.axis_size("sp")
    me = lax.axis_index("sp")
    inner = lax.rem(me, PAIR)
    outer = me // PAIR
    tp_peers = range(1, lax.axis_size("tp"))
    sp_peers = range(1, sp_devices)

    def seq_loads(s):
        return [
            pltpu.make_async_copy(src.at[s], dst.at[s], load_sems.at[n, s])
            for n, (src, dst) in enumerate(((values_hbm, values), (gates_hbm, gates)))
        ]

    table_load = pltpu.make_async_copy(table_hbm, table, misc_sems.at[0])
    row_loads = [
        pltpu.make_async_copy(src, dst, misc_sems.at[n])
        for n, (src, dst) in enumerate(
            ((taps_hbm, taps), (bias_hbm, bias_row), (gain_hbm, gain_row)), 2
        )
    ]
    weight_load = pltpu.make_async_copy(
        weight_hbm, swished.at[:, :width], misc_sems.at[1]
    )

    def strip(i):
        return pl.ds(pl.multiple_of(i * strip_width, strip_width), strip_width)

    def cot_load(i):
        return pltpu.make_async_copy(cot_hbm.at[:, strip(i)], cot.at[:, strip(i)], cot_sems.at[i])

    for copy in row_loads:
        copy.start()
    for copy in seq_loads(0):
        copy.start()
    table_load.start()
    for s in range(1, seqs):
        for copy in seq_loads(s):
            copy.start()
    weight_load.start()

    greet([("tp", d) for d in tp_peers] + [("sp", d) for d in sp_peers])
    last = pl.ds(tokens - HALO, HALO)
    halo_copies = [
        remote(src.at[:, last], dst, halo_send.at[n], halo_recv.at[n], "sp", 1)
        for n, (src, dst) in enumerate(((values_hbm, values_halo), (gates_hbm, gates_halo)))
    ]
    for copy in halo_copies:
        copy.start()

    tail = tokens - (windows - 1) * STEP + HALO
    x_last[tail:, :] = jnp.zeros((SPAN - tail, chans), BF16)
    for ref in (grad_high, grad_low):
        ref[tokens:, :] = jnp.zeros((ref.shape[0] - tokens, chans), BF16)
    for ref in (gain_acc, bias_acc, corr_re, corr_im, tap_rows):
        ref[...] = jnp.zeros_like(ref)
    for copy in row_loads:
        copy.wait()
    tap_rows[:K, :] = taps[...].astype(F32)
    bias = bias_row[...].astype(F32).reshape(1, chans)
    gain = gain_row[...].astype(F32).reshape(1, chans)

    table_load.wait()
    taps_wide = dot(table[TAPF : TAPF + 2 * SPAN], tap_rows[...].astype(BF16))
    taps_wide = taps_wide[:SPAN] + taps_wide[SPAN:]
    for q in range(SPAN // 16):
        tap_re[8 * q : 8 * q + 8, :] = taps_wide[16 * q : 16 * q + 8]
        tap_im[8 * q : 8 * q + 8, :] = taps_wide[16 * q + 8 : 16 * q + 16]

    def gate(values_part, gates_part):
        return (values_part.astype(F32) * sigmoid(gates_part.astype(F32))).astype(BF16)

    def gate_all(s, carry):
        for copy in seq_loads(s):
            copy.wait()
        for i in range(chunks):
            here = slice(i * LANES, (i + 1) * LANES)
            gated = gate(values[s, here, :], gates[s, here, :])
            values[s, here, :] = gated
            count = min(STEP - i * LANES, LANES)
            if count > 0:
                x_first[s, HALO + i * LANES : HALO + i * LANES + count, :] = gated[:count]
        return carry

    lax.fori_loop(0, seqs, gate_all, 0)
    for i in range(strips):
        cot_load(i).start()

    def turn(i, carry):
        here = pl.ds(pl.multiple_of(i * 512, 512), 512)
        weight_t[here, :] = swished[:, here].T
        return carry

    def product(x, sign, high_ref, low_ref):
        for q in range(SPAN // 16):
            a, b = tap_re[8 * q : 8 * q + 8, :], tap_im[8 * q : 8 * q + 8, :]
            re, im = x[16 * q : 16 * q + 8], x[16 * q + 8 : 16 * q + 16]
            if sign > 0:
                both = (a * re - b * im, a * im + b * re)
            else:
                both = (a * re + b * im, a * im - b * re)
            here = slice(16 * q, 16 * q + 16)
            high_ref[here, :], low_ref[here, :] = split(jnp.concatenate(both, axis=0))

    def sums_copies(s):
        return [
            remote(sums.at[s], sums_in.at[d - 1, s], sums_send, sums_recv.at[s], "tp", d)
            for d in tp_peers
        ]

    weight_load.wait()
    lax.fori_loop(0, width // 512, turn, 0)
    for copy in halo_copies:
        copy.wait()
    keep = jnp.where(me > 0, 1.0, 0.0).astype(F32)
    for s in range(seqs):
        x_first[s, :HALO, :] = gate(values_halo[s].astype(F32) * keep, gates_halo[s])

    def ahead(s, carry):
        x_last[:tail, :] = values[s, tokens - tail :, :]
        for w in range(windows):
            if w == 0:
                x = x_first[s]
            elif w < windows - 1:
                x = values[s, w * STEP - HALO : w * STEP + STEP, :]
            else:
                x = x_last[...]
            x = dot(table[FWD : FWD + 2 * SPAN], x)
            x = x[:SPAN] + x[SPAN:]
            spectrum[s * windows + w] = x.astype(BF16)
            product(x, 1, high.at[w], low.at[w])
        for w in range(windows):
            y = dot(table[CONV : CONV + 2 * STEP], high[w])
            y = y[:STEP] + y[STEP:] + dot(table[CONV : CONV + STEP], low[w]) + bias
            count = min(STEP, tokens - w * STEP)
            conv[s, w * STEP : w * STEP + count, :] = y[:count]
        for i in range(chunks):
            total = square = None
            for h in range(lane_blocks):
                part = conv[s, i * LANES : (i + 1) * LANES, h * LANES : (h + 1) * LANES]
                total = part if total is None else total + part
                square = part * part if square is None else square + part * part
            sums[s, 0, i : i + 1, :] = lane_sums(total)
            sums[s, 1, i : i + 1, :] = lane_sums(square)
        for copy in sums_copies(s):
            copy.start()
        return carry

    lax.fori_loop(0, seqs, ahead, 0)
    for s in range(seqs):
        seq_loads(s)[0].start()

    side = 2 if seqs % 2 == 0 else 1
    half_gain = 0.5 * gain

    def norm(p, carry):
        for s in range(side):
            arrive(sums_in.at[:, p * side + s], sums_recv.at[p * side + s], "tp")
        for n in range(side):
            s = p * side + n
            total = sums[s]
            for d in tp_peers:
                total = total + sums_in[d - 1, s]
            mean_rows = total[0] / total_chans
            variance = total[1] / total_chans - mean_rows * mean_rows
            inverse_rows = lax.rsqrt(variance + EPS)
            stat[s] = inverse_rows
            def spreads(i):
                return row_spread(mean_rows[i : i + 1]), row_spread(inverse_rows[i : i + 1])

            following = spreads(0)
            for i in range(chunks):
                here = slice(i * LANES, (i + 1) * LANES)
                columns = pl.ds(pl.multiple_of(s * tokens + i * LANES, LANES), LANES)
                mean, inverse = following
                if i + 1 < chunks:
                    following = spreads(i + 1)
                for h in range(lane_blocks):
                    lanes = slice(h * LANES, (h + 1) * LANES)
                    normed = (conv[s, here, lanes] - mean) * inverse
                    conv[s, here, lanes] = normed
                    half = normed * half_gain[:, lanes]
                    swished[lanes, columns] = (half * jnp.tanh(half) + half).astype(BF16).T
        return carry

    lax.fori_loop(0, seqs // side, norm, 0)

    def part_columns(c):
        return pl.ds(pl.multiple_of(c * part_width, part_width), part_width)

    def pair_copy(c):
        columns = part_columns(c)
        return remote(
            weight_grad.at[1 - inner, :, :, columns], pair.at[:, :, columns], pair_send,
            pair_recv.at[c], "sp", sp_devices + 1 - 2 * inner,
        )

    def onward_copy(d, c):
        columns = part_columns(c)
        return remote(
            onward.at[d - 1, :, columns], arrived.at[d - 1, :, columns], onward_send,
            onward_recv, "sp", d * PAIR,
        )

    def pass_on(c):
        columns = part_columns(c)
        pair_copy(c).wait_recv()
        for d in range(1, groups):
            target = lax.rem(outer + d, groups)
            onward[d - 1, :, columns] = (
                weight_grad[inner, target, :, columns].astype(F32)
                + pair[target, :, columns].astype(F32)
            ).astype(BF16)
        for d in range(1, groups):
            onward_copy(d, c).start()

    def project(i, carry):
        cot_load(i).wait()
        result = dot(swished[:, :positions], cot[:, strip(i)])
        for g in range(groups):
            for n in range(PAIR):
                first = (g * PAIR + n) * weight_rows
                weight_grad[n, g, :, strip(i)] = result[first : first + weight_rows].astype(BF16)
        for n in range(strip_parts):
            pair_copy(i * strip_parts + n).start()

        @pl.when(i >= lag)
        def _():
            pass_on(i - lag)

        return carry

    lag = min(3, strips)
    strip_parts = parts // strips
    lax.fori_loop(0, strips, project, 0)
    passed = strips - lag

    def back_copies(j):
        return [
            remote(back.at[j], back_in.at[d - 1, j], back_send, back_recv.at[j // seq_blocks],
                   "tp", d)
            for d in tp_peers
        ]

    def multiply(j):
        here = pl.ds(pl.multiple_of(j * rows, rows), rows)
        grad[lax.rem(j, 2)] = dot(cot[here, :], weight_t[...])

    def middle(j, following=None):
        s = j // seq_blocks
        first = lax.rem(j, seq_blocks) * rows
        slot = lax.rem(j, 2)
        for i in range(block_chunks):
            here = pl.ds(pl.multiple_of(first + i * LANES, LANES), LANES)
            plain = weighted = None
            for h in range(lane_blocks):
                lanes = slice(h * LANES, (h + 1) * LANES)
                normed = conv[s, here, lanes]
                scaled = normed * gain[:, lanes]
                sig = sigmoid(scaled)
                silu = scaled * sig
                scaled_grad = grad[slot, i * LANES : (i + 1) * LANES, lanes] * (
                    sig + silu * (1.0 - sig)
                )
                normed_grad = scaled_grad * gain[:, lanes]
                norm_grad[s, here, lanes] = normed_grad
                term = scaled_grad * normed
                gain_acc[:, lanes] += jnp.sum(term.reshape(LANES // 8, 8, LANES), axis=0)
                term = normed_grad * normed
                plain = normed_grad if plain is None else plain + normed_grad
                weighted = term if weighted is None else weighted + term
            back[j, 0, i : i + 1, :] = lane_sums(plain)
            back[j, 1, i : i + 1, :] = lane_sums(weighted)
            if following is not None:
                deep = slice(i * width // block_chunks, (i + 1) * width // block_chunks)
                here = pl.ds(pl.multiple_of(following * rows, rows), rows)
                part = dot(cot[here, deep], weight_t[deep, :])
                result = part if i == 0 else result + part
        if following is not None:
            grad[lax.rem(following, 2)] = result
        for copy in back_copies(j):
            copy.start()

    multiply(0)

    def both(j, carry):
        middle(j - 1, j)

        @pl.when(passed + j - 1 < parts)
        def _():
            pass_on(passed + j - 1)

        return carry

    lax.fori_loop(1, blocks, both, 0)
    middle(blocks - 1)
    passed_on = passed + blocks - 1
    if passed_on < parts:
        pass_on(passed_on)
        passed_on += 1

    def grad_copies(s):
        return [
            pltpu.make_async_copy(src.at[s], dst.at[s], misc_sems.at[3 + n])
            for n, (src, dst) in enumerate(((values, values_grad_hbm), (gates, gates_grad_hbm)))
        ]

    def head_copy(s):
        return remote(
            heads.at[s], heads_in.at[s], head_send, head_recv, "sp", sp_devices - 1
        )

    per = tokens // SPAN

    def spread_parts(s, w):
        here = pl.ds(pl.multiple_of(s * tokens + w % per * SPAN, SPAN), SPAN)
        return spectrum.at[s * windows + w], cot.at[here, pl.ds(w // per * chans, chans)]

    def spread_window(s, w):
        high_ref, low_ref = spread_parts(s, w)
        y = dot(table[INV : INV + 2 * SPAN], high_ref[...])
        y = y[:SPAN] + y[SPAN:] + dot(table[INV : INV + SPAN], low_ref[...])
        count = min(STEP, tokens - w * STEP)
        conv[s, w * STEP : w * STEP + count, :] = y[HALO : HALO + count]
        return y[:HALO]

    def behind(s, carry):
        arrive(back_in.at[:, pl.ds(s * seq_blocks, seq_blocks)], back_recv.at[s], "tp")
        for i in range(chunks):
            here = slice(i * LANES, (i + 1) * LANES)
            j = s * seq_blocks + i // block_chunks
            at = slice(i % block_chunks, i % block_chunks + 1)
            inverse_row = stat[s, i : i + 1, :]
            plain, weighted = back[j, 0, at, :], back[j, 1, at, :]
            for d in tp_peers:
                plain = plain + back_in[d - 1, j, 0, at, :]
                weighted = weighted + back_in[d - 1, j, 1, at, :]
            scale = inverse_row / total_chans
            inverse = row_spread(inverse_row)
            plain = row_spread(plain * scale)
            weighted = row_spread(weighted * scale)
            for h in range(lane_blocks):
                lanes = slice(h * LANES, (h + 1) * LANES)
                conv_grad = inverse * norm_grad[s, here, lanes] - plain - conv[s, here, lanes] * weighted
                grad_high[here, lanes], grad_low[here, lanes] = split(conv_grad)
                bias_acc[:, lanes] += jnp.sum(conv_grad.reshape(LANES // 8, 8, LANES), axis=0)
        for w in range(windows):
            here = slice(w * STEP, w * STEP + SPAN)
            g = dot(table[GRAD : GRAD + 2 * SPAN], grad_high[here, :])
            g = g[:SPAN] + g[SPAN:] + dot(table[GRAD : GRAD + SPAN], grad_low[here, :])
            x = spectrum[s * windows + w].astype(F32)
            for q in range(SPAN // 16):
                at = slice(8 * q, 8 * q + 8)
                g_re, g_im = g[16 * q : 16 * q + 8], g[16 * q + 8 : 16 * q + 16]
                x_re, x_im = x[16 * q : 16 * q + 8], x[16 * q + 8 : 16 * q + 16]
                corr_re[at, :] += g_re * x_re + g_im * x_im
                corr_im[at, :] += g_im * x_re - g_re * x_im
            product(g, -1, *spread_parts(s, w))
            if w == 0:
                heads[s] = spread_window(s, 0).astype(BF16)
        head_copy(s).start()

        @pl.when(passed_on + s < parts)
        def _():
            pass_on(passed_on + s)

        return carry

    lax.fori_loop(0, seqs, behind, 0)

    corr = []
    for q in range(SPAN // 16):
        corr += [corr_re[8 * q : 8 * q + 8, :], corr_im[8 * q : 8 * q + 8, :]]
    corr_high, corr_low = split(jnp.concatenate(corr, axis=0))
    taps_grad = dot(table[TAPI : TAPI + 64], corr_high)
    taps_grad = taps_grad[:32] + taps_grad[32:] + dot(table[TAPI : TAPI + 32], corr_low)
    small[:32, :] = taps_grad
    small[32:33, :] = jnp.sum(bias_acc[...], axis=0, keepdims=True)
    small[33:34, :] = jnp.sum(gain_acc[...], axis=0, keepdims=True)
    small[34:, :] = jnp.zeros((small.shape[0] - 34, chans), F32)
    small_pair = remote(
        small, small_in.at[0], pair_send, small_recv.at[0], "sp",
        sp_devices + 1 - 2 * inner,
    )
    small_pair.start()
    for c in range(min(passed_on + seqs, parts), parts):
        pass_on(c)

    def spread_rest(s, carry):
        for w in range(1, windows):
            conv[s, w * STEP - HALO : w * STEP, :] += spread_window(s, w)
        return carry

    lax.fori_loop(0, seqs, spread_rest, 0)
    small_pair.wait_recv()
    small_sum[...] = small[...] + small_in[0]
    small_copies = [
        remote(small_sum, small_in.at[d], small_send, small_recv.at[1], "sp", d * PAIR)
        for d in range(1, groups)
    ]
    for copy in small_copies:
        copy.start()
    keep_head = jnp.where(me < sp_devices - 1, 1.0, 0.0).astype(F32)
    arrive(heads_in, head_recv, "sp")
    for s in range(seqs):
        seq_loads(s)[0].wait()

    def finish(s, carry):
        conv[s, tokens - HALO :, :] += heads_in[s].astype(F32) * keep_head
        for i in range(chunks):
            here = slice(i * LANES, (i + 1) * LANES)
            sig = sigmoid(gates[s, here, :].astype(F32))
            values_part = conv[s, here, :] * sig
            gates_part = values_part * values[s, here, :].astype(F32) * (1.0 - sig)
            values[s, here, :] = values_part.astype(BF16)
            gates[s, here, :] = gates_part.astype(BF16)
        for copy in grad_copies(s):
            copy.start()
        return carry

    lax.fori_loop(0, seqs, finish, 0)

    arrive(arrived, onward_recv, "sp")
    for c in range(parts):
        columns = slice(c * part_width, (c + 1) * part_width)
        result = weight_grad[inner, outer, :, columns].astype(F32)
        result = result + pair[outer, :, columns].astype(F32)
        for d in range(1, groups):
            result = result + arrived[d - 1, :, columns].astype(F32)
        weight_sum[:, columns] = result
        if (c + 1) % strip_parts == 0:
            columns = pl.ds(c // strip_parts * strip_width, strip_width)
            pltpu.make_async_copy(
                weight_sum.at[:, columns], weight_out_hbm.at[:, columns], misc_sems.at[2]
            ).start()
    arrive(small_in.at[1:], small_recv.at[1], "sp")
    total = small_sum[...]
    for d in range(1, groups):
        total = total + small_in[d]
    small_total[...] = total
    outs = [pltpu.make_async_copy(small_total, small_hbm, misc_sems.at[1])]
    outs[0].start()
    for ref, sem, axis in (
        (sums_in, sums_send, "tp"), (back_in, back_send, "tp"), (onward, onward_send, "sp"),
        (pair, pair_send, "sp"), (small, pair_send, "sp"), (heads, head_send, "sp"),
        (small_in.at[1:], small_send, "sp"),
    ):
        remote(ref, ref, sem, sem, axis, 1).wait_send()
    outs.append(pltpu.make_async_copy(weight_sum, weight_out_hbm, misc_sems.at[2]))
    outs.append(pltpu.make_async_copy(values, values_grad_hbm, misc_sems.at[3]))
    outs.append(pltpu.make_async_copy(gates, gates_grad_hbm, misc_sems.at[4]))
    for copy in outs:
        copy.wait()


def hand_over_kernel(
    values_hbm, gates_hbm, weight_hbm, small_hbm,
    values_grad_hbm, gates_grad_hbm, weight_grad_hbm, taps_grad_hbm, gain_grad_hbm, bias_grad_hbm,
    values, gates, weight, small, taps_grad, gain_grad, bias_grad, in_sems, out_sems,
):
    seqs = values.shape[0]
    pairs = [(small_hbm, small, None)]
    for s in range(seqs):
        pairs.append((values_hbm.at[s], values.at[s], values_grad_hbm.at[s]))
        pairs.append((gates_hbm.at[s], gates.at[s], gates_grad_hbm.at[s]))
    pairs.append((weight_hbm, weight, weight_grad_hbm))
    loads = [
        pltpu.make_async_copy(src, here, in_sems.at[n]) for n, (src, here, _) in enumerate(pairs)
    ]
    for copy in loads:
        copy.start()
    stores = []

    def store(here, dst):
        stores.append(pltpu.make_async_copy(here, dst, out_sems.at[len(stores)]))
        stores[-1].start()

    for copy, (_, here, dst) in zip(loads[1:], pairs[1:]):
        copy.wait()
        store(here, dst)
    loads[0].wait()
    taps_grad[...] = small[:K]
    bias_grad[...] = small[32:33]
    gain_grad[...] = small[33:34]
    store(taps_grad, taps_grad_hbm)
    store(gain_grad, gain_grad_hbm)
    store(bias_grad, bias_grad_hbm)
    for copy in stores:
        copy.wait()


def on_device(values_in, gates_in, conv_taps, conv_bias, norm_gain, out_weight, out_grad):
    seqs, tokens, chans = values_in.shape
    width = out_grad.shape[2]
    total_chans = chans * lax.axis_size("tp")
    positions = seqs * tokens
    rows = min(512, tokens)
    blocks = positions // rows
    chunks = tokens // LANES
    windows = -(-tokens // STEP)
    strips = 8
    parts = 16
    tp_others = lax.axis_size("tp") - 1
    sp_devices = lax.axis_size("sp")
    groups = sp_devices // PAIR
    weight_rows = chans // sp_devices
    small_rows = 40

    def dma(*shape):
        return pltpu.SemaphoreType.DMA(shape)

    one = pltpu.SemaphoreType.DMA
    anywhere = pl.BlockSpec(memory_space=pl.ANY)
    padded = windows * STEP + HALO
    block_sums = (2, rows // LANES, LANES)
    values_sum, gates_sum, small, weight_sum = pl.pallas_call(
        functools.partial(fused_kernel, total_chans),
        in_specs=[anywhere] * 8,
        out_specs=[anywhere] * 4,
        out_shape=[
            jax.ShapeDtypeStruct((seqs, tokens, chans), BF16),
            jax.ShapeDtypeStruct((seqs, tokens, chans), BF16),
            jax.ShapeDtypeStruct((small_rows, chans), F32),
            jax.ShapeDtypeStruct((weight_rows, width), F32),
        ],
        scratch_shapes=[
            pltpu.VMEM((seqs, tokens, chans), BF16),
            pltpu.VMEM((seqs, tokens, chans), BF16),
            pltpu.VMEM((seqs, HALO, chans), BF16),
            pltpu.VMEM((seqs, HALO, chans), BF16),
            pltpu.VMEM((positions, width), BF16),
            pltpu.VMEM((chans, max(positions, width)), BF16),
            pltpu.VMEM((width, chans), BF16),
            pltpu.VMEM((PAIR, groups, weight_rows, width), BF16),
            pltpu.VMEM((groups, weight_rows, width), BF16),
            pltpu.VMEM((groups - 1, weight_rows, width), BF16),
            pltpu.VMEM((groups - 1, weight_rows, width), BF16),
            pltpu.VMEM((weight_rows, width), F32),
            pltpu.VMEM((seqs, tokens, chans), F32),
            pltpu.VMEM((seqs, tokens, chans), F32),
            pltpu.VMEM((2, rows, chans), F32),
            pltpu.VMEM((seqs, SPAN, chans), BF16),
            pltpu.VMEM((SPAN, chans), BF16),
            pltpu.VMEM((seqs * windows, SPAN, chans), BF16),
            pltpu.VMEM((windows, SPAN, chans), BF16),
            pltpu.VMEM((windows, SPAN, chans), BF16),
            pltpu.VMEM((padded, chans), BF16),
            pltpu.VMEM((padded, chans), BF16),
            pltpu.VMEM((TABLE_ROWS, SPAN), BF16),
            pltpu.VMEM((K, chans), BF16),
            pltpu.VMEM((chans,), BF16),
            pltpu.VMEM((chans,), BF16),
            pltpu.VMEM((SPAN, chans), F32),
            pltpu.VMEM((SPAN // 2, chans), F32),
            pltpu.VMEM((SPAN // 2, chans), F32),
            pltpu.VMEM((SPAN // 2, chans), F32),
            pltpu.VMEM((SPAN // 2, chans), F32),
            pltpu.VMEM((seqs, HALO, chans), BF16),
            pltpu.VMEM((seqs, HALO, chans), BF16),
            pltpu.VMEM((seqs, 2, chunks, LANES), F32),
            pltpu.VMEM((tp_others, seqs, 2, chunks, LANES), F32),
            pltpu.VMEM((seqs, chunks, LANES), F32),
            pltpu.VMEM((blocks, *block_sums), F32),
            pltpu.VMEM((tp_others, blocks, *block_sums), F32),
            pltpu.VMEM((8, chans), F32),
            pltpu.VMEM((8, chans), F32),
            pltpu.VMEM((small_rows, chans), F32),
            pltpu.VMEM((small_rows, chans), F32),
            pltpu.VMEM((small_rows, chans), F32),
            pltpu.VMEM((groups, small_rows, chans), F32),
            dma(2, seqs),
            dma(strips),
            dma(5),
            dma(2),
            dma(2),
            one,
            dma(seqs),
            one,
            dma(seqs),
            one,
            dma(parts),
            one,
            one,
            one,
            one,
            one,
            dma(2),
        ],
        compiler_params=pltpu.CompilerParams(
            vmem_limit_bytes=VMEM_LIMIT, collective_id=0, has_side_effects=True
        ),
        name="fused",
    )(
        values_in, gates_in, out_grad.reshape(positions, width), out_weight,
        jnp.asarray(transform_table()), conv_taps, conv_bias, norm_gain,
    )

    values_grad, gates_grad, weight_grad, taps_grad, gain_grad, bias_grad = pl.pallas_call(
        hand_over_kernel,
        in_specs=[anywhere] * 4,
        out_specs=[anywhere] * 6,
        out_shape=[
            jax.ShapeDtypeStruct((seqs, tokens, chans), BF16),
            jax.ShapeDtypeStruct((seqs, tokens, chans), BF16),
            jax.ShapeDtypeStruct((weight_rows, width), F32),
            jax.ShapeDtypeStruct((K, chans), F32),
            jax.ShapeDtypeStruct((1, chans), F32),
            jax.ShapeDtypeStruct((1, chans), F32),
        ],
        scratch_shapes=[
            pltpu.VMEM((seqs, tokens, chans), BF16),
            pltpu.VMEM((seqs, tokens, chans), BF16),
            pltpu.VMEM((weight_rows, width), F32),
            pltpu.VMEM((small_rows, chans), F32),
            pltpu.VMEM((K, chans), F32),
            pltpu.VMEM((1, chans), F32),
            pltpu.VMEM((1, chans), F32),
            dma(2 * seqs + 2),
            dma(2 * seqs + 4),
        ],
        compiler_params=pltpu.CompilerParams(vmem_limit_bytes=VMEM_LIMIT),
        name="hand_over",
    )(values_sum, gates_sum, weight_sum, small)
    return values_grad, gates_grad, taps_grad, gain_grad[0], bias_grad[0], weight_grad


def solution(mesh):
    return jax.shard_map(
        on_device,
        mesh=mesh,
        in_specs=(
            P(None, "sp", "tp"),
            P(None, "sp", "tp"),
            P(None, "tp"),
            P("tp"),
            P("tp"),
            P("tp", None),
            P(None, "sp", None),
        ),
        out_specs=(
            P(None, "sp", "tp"),
            P(None, "sp", "tp"),
            P(None, "tp"),
            P("tp"),
            P("tp"),
            P(("tp", "sp"), None),
        ),
        check_vma=False,
    )
```

```python
import functools

import jax
import jax.numpy as jnp
import numpy as np
from jax import lax
from jax.experimental import pallas as pl
from jax.experimental.pallas import tpu as pltpu
from jax.sharding import PartitionSpec as P

K = 31
EPS = 1e-05
HALO = 32
PAIR = 2
LAG = 4
LANES = 128
SPAN = 256
STEP = SPAN - HALO
F32 = jnp.float32
BF16 = jnp.bfloat16
VMEM_LIMIT = 64 * 1024 * 1024 - 64 * 1024

FWD, GRAD, INV, CONV, TAPF, TAPI = 0, 512, 1024, 1536, 1984, 2496
TABLE_ROWS = 2560


def transform_table():
    row = np.arange(SPAN)
    freq = 8 * (row // 16) + row % 8
    angle = 2 * np.pi * (freq[:, None] + 0.5) * np.arange(SPAN)[None] / SPAN
    fwd = np.where((row // 8 % 2 == 0)[:, None], np.cos(angle), -np.sin(angle))
    inv = fwd.T * (2 / SPAN)
    grad = np.zeros((SPAN, SPAN))
    grad[:, :STEP] = fwd[:, HALO:]
    tap_fwd = np.zeros((SPAN, SPAN))
    tap_fwd[:, :K] = fwd[:, K - 1 :: -1]
    tap_inv = np.zeros((32, SPAN))
    tap_inv[:K] = inv[K - 1 :: -1]
    parts = []
    for whole_part in (fwd, grad, inv, inv[HALO:], tap_fwd, tap_inv):
        high = whole_part.astype(BF16)
        parts += [high, (whole_part - high.astype(np.float64)).astype(BF16)]
    return np.concatenate(parts)


def sigmoid(x):
    return 0.5 * jnp.tanh(0.5 * x) + 0.5


def peer_id(axis, distance):
    devices = lax.axis_size(axis)
    return {axis: lax.rem(lax.axis_index(axis) + distance, devices)}


def greet(pairs):
    barrier = pltpu.get_barrier_semaphore()
    for axis, distance in pairs:
        pl.semaphore_signal(
            barrier, inc=1, device_id=peer_id(axis, distance),
            device_id_type=pl.DeviceIdType.MESH,
        )
    pl.semaphore_wait(barrier, len(pairs))


def remote(src, dst, send_sem, recv_sem, axis, distance):
    return pltpu.make_async_remote_copy(
        src_ref=src, dst_ref=dst, send_sem=send_sem, recv_sem=recv_sem,
        device_id=peer_id(axis, distance), device_id_type=pl.DeviceIdType.MESH,
    )


def arrive(ref, sem, axis):
    remote(ref, ref, sem, sem, axis, 1).wait_recv()


def dot(a, b):
    return jnp.dot(a, b, preferred_element_type=F32)


def lane_sums(x):
    return jnp.sum(x.T, axis=0, keepdims=True)


def row_spread(row):
    return jnp.broadcast_to(row, (LANES, LANES)).T


def split(x):
    high = x.astype(BF16)
    return high, (x - high.astype(F32)).astype(BF16)


def fused_kernel(
    total_chans, values_hbm, gates_hbm, cot_hbm, weight_hbm, table_hbm, taps_hbm, bias_hbm,
    gain_hbm,
    values_grad_hbm, gates_grad_hbm, small_hbm, weight_out_hbm,
    values, gates, values_halo, gates_halo, cot, swished, weight_t, weight_grad, pair,
    onward, arrived, weight_sum, conv, norm_grad, grad, x_first, x_last, spectrum, high, low, grad_high, grad_low, table,
    taps, bias_row, gain_row, tap_rows,
    tap_re, tap_im, corr_re, corr_im, heads, heads_in, sums, sums_in, stat, back, back_in,
    gain_acc, bias_acc, small, small_sum, small_in,
    load_sems, cot_sems, misc_sems, halo_send, halo_recv, sums_send, sums_recv,
    back_send, back_recv, pair_send, pair_recv, onward_send, onward_recv, head_send, head_recv,
    small_send, small_recv,
):
    seqs, tokens, chans = values.shape
    positions, width = cot.shape
    lane_blocks = chans // LANES
    chunks = tokens // LANES
    windows = spectrum.shape[0] // seqs
    rows = grad.shape[1]
    blocks = positions // rows
    strips = cot_sems.shape[0]
    strip_width = width // strips
    seq_blocks = blocks // seqs
    block_chunks = rows // LANES
    parts = pair_recv.shape[0]
    part_width = width // parts
    groups, weight_rows = pair.shape[0], pair.shape[1]
    sp_devices = lax.axis_size("sp")
    me = lax.axis_index("sp")
    inner = lax.rem(me, PAIR)
    outer = me // PAIR
    tp_peers = range(1, lax.axis_size("tp"))
    sp_peers = range(1, sp_devices)

    def seq_loads(s):
        return [
            pltpu.make_async_copy(src.at[s], dst.at[s], load_sems.at[n, s])
            for n, (src, dst) in enumerate(((values_hbm, values), (gates_hbm, gates)))
        ]

    table_load = pltpu.make_async_copy(table_hbm, table, misc_sems.at[0])
    row_loads = [
        pltpu.make_async_copy(src, dst, misc_sems.at[n])
        for n, (src, dst) in enumerate(
            ((taps_hbm, taps), (bias_hbm, bias_row), (gain_hbm, gain_row)), 2
        )
    ]
    weight_load = pltpu.make_async_copy(
        weight_hbm, swished.at[:, :width], misc_sems.at[1]
    )

    def strip(i):
        return pl.ds(pl.multiple_of(i * strip_width, strip_width), strip_width)

    def cot_load(i):
        return pltpu.make_async_copy(cot_hbm.at[:, strip(i)], cot.at[:, strip(i)], cot_sems.at[i])

    for copy in row_loads:
        copy.start()
    for copy in seq_loads(0):
        copy.start()
    table_load.start()
    for s in range(1, seqs):
        for copy in seq_loads(s):
            copy.start()
    weight_load.start()

    greet([("tp", d) for d in tp_peers] + [("sp", d) for d in sp_peers])
    last = pl.ds(tokens - HALO, HALO)
    halo_pairs = ((values_hbm, values_halo), (gates_hbm, gates_halo))

    def halo_copies(s):
        return [
            remote(src.at[s, last], dst.at[s], halo_send.at[n], halo_recv.at[n, s], "sp", 1)
            for n, (src, dst) in enumerate(halo_pairs)
        ]

    for s in range(seqs):
        for copy in halo_copies(s):
            copy.start()

    tail = tokens - (windows - 1) * STEP + HALO
    x_last[tail:, :] = jnp.zeros((SPAN - tail, chans), BF16)
    for ref in (grad_high, grad_low):
        ref[tokens:, :] = jnp.zeros((ref.shape[0] - tokens, chans), BF16)
    for ref in (gain_acc, bias_acc, corr_re, corr_im, tap_rows):
        ref[...] = jnp.zeros_like(ref)
    for copy in row_loads:
        copy.wait()
    tap_rows[:K, :] = taps[...].astype(F32)
    bias = bias_row[...].astype(F32).reshape(1, chans)
    gain = gain_row[...].astype(F32).reshape(1, chans)

    table_load.wait()
    taps_wide = dot(table[TAPF : TAPF + 2 * SPAN], tap_rows[...].astype(BF16))
    taps_wide = taps_wide[:SPAN] + taps_wide[SPAN:]
    for q in range(SPAN // 16):
        tap_re[8 * q : 8 * q + 8, :] = taps_wide[16 * q : 16 * q + 8]
        tap_im[8 * q : 8 * q + 8, :] = taps_wide[16 * q + 8 : 16 * q + 16]

    def gate(values_part, gates_part):
        return (values_part.astype(F32) * sigmoid(gates_part.astype(F32))).astype(BF16)

    def gate_all(s, carry):
        for copy in seq_loads(s):
            copy.wait()
        for i in range(chunks):
            here = slice(i * LANES, (i + 1) * LANES)
            gated = gate(values[s, here, :], gates[s, here, :])
            values[s, here, :] = gated
            count = min(STEP - i * LANES, LANES)
            if count > 0:
                x_first[s, HALO + i * LANES : HALO + i * LANES + count, :] = gated[:count]
        return carry

    lax.fori_loop(0, seqs, gate_all, 0)
    for i in range(strips):
        cot_load(i).start()

    def turn(i, carry):
        here = pl.ds(pl.multiple_of(i * 512, 512), 512)
        weight_t[here, :] = swished[:, here].T
        return carry

    def product(x, sign, high_ref, low_ref):
        for q in range(SPAN // 16):
            a, b = tap_re[8 * q : 8 * q + 8, :], tap_im[8 * q : 8 * q + 8, :]
            re, im = x[16 * q : 16 * q + 8], x[16 * q + 8 : 16 * q + 16]
            if sign > 0:
                both = (a * re - b * im, a * im + b * re)
            else:
                both = (a * re + b * im, a * im - b * re)
            here = slice(16 * q, 16 * q + 16)
            high_ref[here, :], low_ref[here, :] = split(jnp.concatenate(both, axis=0))

    def sums_copies(s):
        return [
            remote(sums.at[s], sums_in.at[d - 1, s], sums_send, sums_recv.at[s], "tp", d)
            for d in tp_peers
        ]

    weight_load.wait()
    lax.fori_loop(0, width // 512, turn, 0)
    keep = jnp.where(me > 0, 1.0, 0.0).astype(F32)

    def ahead(s, carry):
        for copy in halo_copies(s):
            copy.wait_recv()
        x_first[s, :HALO, :] = gate(values_halo[s].astype(F32) * keep, gates_halo[s])
        x_last[:tail, :] = values[s, tokens - tail :, :]
        for w in range(windows):
            if w == 0:
                x = x_first[s]
            elif w < windows - 1:
                x = values[s, w * STEP - HALO : w * STEP + STEP, :]
            else:
                x = x_last[...]
            x = dot(table[FWD : FWD + 2 * SPAN], x)
            x = x[:SPAN] + x[SPAN:]
            spectrum[s * windows + w] = x.astype(BF16)
            product(x, 1, high.at[w], low.at[w])
        for w in range(windows):
            y = dot(table[CONV : CONV + 2 * STEP], high[w])
            y = y[:STEP] + y[STEP:] + dot(table[CONV : CONV + STEP], low[w]) + bias
            count = min(STEP, tokens - w * STEP)
            conv[s, w * STEP : w * STEP + count, :] = y[:count]
        for i in range(chunks):
            total = square = None
            for h in range(lane_blocks):
                part = conv[s, i * LANES : (i + 1) * LANES, h * LANES : (h + 1) * LANES]
                total = part if total is None else total + part
                square = part * part if square is None else square + part * part
            sums[s, 0, i : i + 1, :] = lane_sums(total)
            sums[s, 1, i : i + 1, :] = lane_sums(square)
        for copy in sums_copies(s):
            copy.start()
        return carry

    lax.fori_loop(0, seqs, ahead, 0)
    for s in range(seqs):
        seq_loads(s)[0].start()

    side = 2 if seqs % 2 == 0 else 1
    half_gain = 0.5 * gain

    def norm(p, carry):
        for s in range(side):
            arrive(sums_in.at[:, p * side + s], sums_recv.at[p * side + s], "tp")
        for n in range(side):
            s = p * side + n
            total = sums[s]
            for d in tp_peers:
                total = total + sums_in[d - 1, s]
            mean_rows = total[0] / total_chans
            variance = total[1] / total_chans - mean_rows * mean_rows
            inverse_rows = lax.rsqrt(variance + EPS)
            stat[s] = inverse_rows
            def spreads(i):
                return row_spread(mean_rows[i : i + 1]), row_spread(inverse_rows[i : i + 1])

            following = spreads(0)
            for i in range(chunks):
                here = slice(i * LANES, (i + 1) * LANES)
                columns = pl.ds(pl.multiple_of(s * tokens + i * LANES, LANES), LANES)
                mean, inverse = following
                if i + 1 < chunks:
                    following = spreads(i + 1)
                for h in range(lane_blocks):
                    lanes = slice(h * LANES, (h + 1) * LANES)
                    normed = (conv[s, here, lanes] - mean) * inverse
                    conv[s, here, lanes] = normed
                    half = normed * half_gain[:, lanes]
                    swished[lanes, columns] = (half * jnp.tanh(half) + half).astype(BF16).T
        return carry

    lax.fori_loop(0, seqs // side, norm, 0)

    def part_columns(c):
        return pl.ds(pl.multiple_of(c * part_width, part_width), part_width)

    def pair_copy(c):
        columns = part_columns(c)
        return remote(
            weight_grad.at[1 - inner, :, :, columns], pair.at[:, :, columns], pair_send,
            pair_recv.at[c], "sp", sp_devices + 1 - 2 * inner,
        )

    def onward_copy(d, c):
        columns = part_columns(c)
        return remote(
            onward.at[d - 1, :, columns], arrived.at[d - 1, :, columns], onward_send,
            onward_recv, "sp", d * PAIR,
        )

    def pass_on(c):
        columns = part_columns(c)
        pair_copy(c).wait_recv()
        for d in range(1, groups):
            target = lax.rem(outer + d, groups)
            onward[d - 1, :, columns] = (
                weight_grad[inner, target, :, columns].astype(F32)
                + pair[target, :, columns].astype(F32)
            ).astype(BF16)
        for d in range(1, groups):
            onward_copy(d, c).start()

    def project(i, carry):
        cot_load(i).wait()
        result = dot(swished[:, :positions], cot[:, strip(i)])
        for g in range(groups):
            for n in range(PAIR):
                first = (g * PAIR + n) * weight_rows
                weight_grad[n, g, :, strip(i)] = result[first : first + weight_rows].astype(BF16)
        for n in range(strip_parts):
            pair_copy(i * strip_parts + n).start()

        @pl.when(i >= lag)
        def _():
            pass_on(i - lag)

        return carry

    lag = min(LAG, strips)
    strip_parts = parts // strips
    lax.fori_loop(0, strips, project, 0)
    passed = strips - lag

    def back_copies(j):
        return [
            remote(back.at[j], back_in.at[d - 1, j], back_send, back_recv.at[j // seq_blocks],
                   "tp", d)
            for d in tp_peers
        ]

    def multiply(j):
        here = pl.ds(pl.multiple_of(j * rows, rows), rows)
        grad[lax.rem(j, 2)] = dot(cot[here, :], weight_t[...])

    def middle(j, following=None):
        s = j // seq_blocks
        first = lax.rem(j, seq_blocks) * rows
        slot = lax.rem(j, 2)
        for i in range(block_chunks):
            here = pl.ds(pl.multiple_of(first + i * LANES, LANES), LANES)
            plain = weighted = None
            for h in range(lane_blocks):
                lanes = slice(h * LANES, (h + 1) * LANES)
                normed = conv[s, here, lanes]
                scaled = normed * gain[:, lanes]
                sig = sigmoid(scaled)
                silu = scaled * sig
                scaled_grad = grad[slot, i * LANES : (i + 1) * LANES, lanes] * (
                    sig + silu * (1.0 - sig)
                )
                normed_grad = scaled_grad * gain[:, lanes]
                norm_grad[s, here, lanes] = normed_grad
                term = scaled_grad * normed
                gain_acc[:, lanes] += jnp.sum(term.reshape(LANES // 8, 8, LANES), axis=0)
                term = normed_grad * normed
                plain = normed_grad if plain is None else plain + normed_grad
                weighted = term if weighted is None else weighted + term
            back[j, 0, i : i + 1, :] = lane_sums(plain)
            back[j, 1, i : i + 1, :] = lane_sums(weighted)
            if following is not None:
                deep = slice(i * width // block_chunks, (i + 1) * width // block_chunks)
                here = pl.ds(pl.multiple_of(following * rows, rows), rows)
                part = dot(cot[here, deep], weight_t[deep, :])
                result = part if i == 0 else result + part
        if following is not None:
            grad[lax.rem(following, 2)] = result
        for copy in back_copies(j):
            copy.start()

    multiply(0)
    if passed < parts:
        pass_on(passed)
        passed += 1

    def both(j, carry):
        middle(j - 1, j)

        @pl.when(passed + j - 1 < parts)
        def _():
            pass_on(passed + j - 1)

        return carry

    lax.fori_loop(1, blocks, both, 0)
    middle(blocks - 1)
    passed_on = passed + blocks - 1
    if passed_on < parts:
        pass_on(passed_on)
        passed_on += 1

    def grad_copies(s):
        return [
            pltpu.make_async_copy(src.at[s], dst.at[s], misc_sems.at[3 + n])
            for n, (src, dst) in enumerate(((values, values_grad_hbm), (gates, gates_grad_hbm)))
        ]

    def head_copy(s):
        return remote(
            heads.at[s], heads_in.at[s], head_send, head_recv, "sp", sp_devices - 1
        )

    per = tokens // SPAN

    def spread_parts(s, w):
        here = pl.ds(pl.multiple_of(s * tokens + w % per * SPAN, SPAN), SPAN)
        return spectrum.at[s * windows + w], cot.at[here, pl.ds(w // per * chans, chans)]

    def spread_window(s, w):
        high_ref, low_ref = spread_parts(s, w)
        y = dot(table[INV : INV + 2 * SPAN], high_ref[...])
        y = y[:SPAN] + y[SPAN:] + dot(table[INV : INV + SPAN], low_ref[...])
        count = min(STEP, tokens - w * STEP)
        conv[s, w * STEP : w * STEP + count, :] = y[HALO : HALO + count]
        return y[:HALO]

    def behind(s, carry):
        arrive(back_in.at[:, pl.ds(s * seq_blocks, seq_blocks)], back_recv.at[s], "tp")
        for i in range(chunks):
            here = slice(i * LANES, (i + 1) * LANES)
            j = s * seq_blocks + i // block_chunks
            at = slice(i % block_chunks, i % block_chunks + 1)
            inverse_row = stat[s, i : i + 1, :]
            plain, weighted = back[j, 0, at, :], back[j, 1, at, :]
            for d in tp_peers:
                plain = plain + back_in[d - 1, j, 0, at, :]
                weighted = weighted + back_in[d - 1, j, 1, at, :]
            scale = inverse_row / total_chans
            inverse = row_spread(inverse_row)
            plain = row_spread(plain * scale)
            weighted = row_spread(weighted * scale)
            for h in range(lane_blocks):
                lanes = slice(h * LANES, (h + 1) * LANES)
                conv_grad = inverse * norm_grad[s, here, lanes] - plain - conv[s, here, lanes] * weighted
                grad_high[here, lanes], grad_low[here, lanes] = split(conv_grad)
                bias_acc[:, lanes] += jnp.sum(conv_grad.reshape(LANES // 8, 8, LANES), axis=0)
        for w in range(windows):
            here = slice(w * STEP, w * STEP + SPAN)
            g = dot(table[GRAD : GRAD + 2 * SPAN], grad_high[here, :])
            g = g[:SPAN] + g[SPAN:] + dot(table[GRAD : GRAD + SPAN], grad_low[here, :])
            x = spectrum[s * windows + w].astype(F32)
            for q in range(SPAN // 16):
                at = slice(8 * q, 8 * q + 8)
                g_re, g_im = g[16 * q : 16 * q + 8], g[16 * q + 8 : 16 * q + 16]
                x_re, x_im = x[16 * q : 16 * q + 8], x[16 * q + 8 : 16 * q + 16]
                corr_re[at, :] += g_re * x_re + g_im * x_im
                corr_im[at, :] += g_im * x_re - g_re * x_im
            product(g, -1, *spread_parts(s, w))
            if w == 0:
                heads[s] = spread_window(s, 0).astype(BF16)
        head_copy(s).start()

        @pl.when(passed_on + s < parts)
        def _():
            pass_on(passed_on + s)

        return carry

    lax.fori_loop(0, seqs, behind, 0)

    corr = []
    for q in range(SPAN // 16):
        corr += [corr_re[8 * q : 8 * q + 8, :], corr_im[8 * q : 8 * q + 8, :]]
    corr_high, corr_low = split(jnp.concatenate(corr, axis=0))
    taps_grad = dot(table[TAPI : TAPI + 64], corr_high)
    taps_grad = taps_grad[:32] + taps_grad[32:] + dot(table[TAPI : TAPI + 32], corr_low)
    small[:32, :] = taps_grad
    small[32:33, :] = jnp.sum(bias_acc[...], axis=0, keepdims=True)
    small[33:34, :] = jnp.sum(gain_acc[...], axis=0, keepdims=True)
    small[34:, :] = jnp.zeros((small.shape[0] - 34, chans), F32)
    small_pair = remote(
        small, small_in, pair_send, small_recv.at[0], "sp",
        sp_devices + 1 - 2 * inner,
    )
    small_pair.start()
    for c in range(min(passed_on + seqs, parts), parts):
        pass_on(c)

    def spread_rest(s, carry):
        for w in range(1, windows):
            conv[s, w * STEP - HALO : w * STEP, :] += spread_window(s, w)
        return carry

    lax.fori_loop(0, seqs, spread_rest, 0)
    small_pair.wait_recv()
    small_sum[...] = (small[...] + small_in[...]).astype(BF16)
    small_copies = []
    for n in range(1, groups):
        d = jnp.where(outer < groups // 2, groups - n, n)
        small_copies.append(
            remote(small_sum, small_hbm.at[d], small_send, small_recv.at[1], "sp", d * PAIR)
        )
    for copy in small_copies:
        copy.start()
    keep_head = jnp.where(me < sp_devices - 1, 1.0, 0.0).astype(F32)
    arrive(heads_in, head_recv, "sp")
    for s in range(seqs):
        seq_loads(s)[0].wait()

    def finish(s, carry):
        conv[s, tokens - HALO :, :] += heads_in[s].astype(F32) * keep_head
        for i in range(chunks):
            here = slice(i * LANES, (i + 1) * LANES)
            sig = sigmoid(gates[s, here, :].astype(F32))
            values_part = conv[s, here, :] * sig
            gates_part = values_part * values[s, here, :].astype(F32) * (1.0 - sig)
            values[s, here, :] = values_part.astype(BF16)
            gates[s, here, :] = gates_part.astype(BF16)
        for copy in grad_copies(s):
            copy.start()
        return carry

    lax.fori_loop(0, seqs, finish, 0)

    arrive(arrived, onward_recv, "sp")
    for c in range(parts):
        columns = slice(c * part_width, (c + 1) * part_width)
        result = weight_grad[inner, outer, :, columns].astype(F32)
        result = result + pair[outer, :, columns].astype(F32)
        for d in range(1, groups):
            result = result + arrived[d - 1, :, columns].astype(F32)
        weight_sum[:, columns] = result
        if (c + 1) % strip_parts == 0:
            columns = pl.ds(c // strip_parts * strip_width, strip_width)
            pltpu.make_async_copy(
                weight_sum.at[:, columns], weight_out_hbm.at[:, columns], misc_sems.at[2]
            ).start()
    outs = [pltpu.make_async_copy(small_sum, small_hbm.at[0], misc_sems.at[1])]
    outs[0].start()
    for ref, sem, axis in (
        (values_halo, halo_send.at[0], "sp"), (gates_halo, halo_send.at[1], "sp"),
        (sums_in, sums_send, "tp"), (back_in, back_send, "tp"), (onward, onward_send, "sp"),
        (pair, pair_send, "sp"), (small, pair_send, "sp"), (heads, head_send, "sp"),
        (small_hbm.at[1:], small_send, "sp"),
    ):
        remote(ref, ref, sem, sem, axis, 1).wait_send()
    outs.append(pltpu.make_async_copy(weight_sum, weight_out_hbm, misc_sems.at[2]))
    outs.append(pltpu.make_async_copy(values, values_grad_hbm, misc_sems.at[3]))
    outs.append(pltpu.make_async_copy(gates, gates_grad_hbm, misc_sems.at[4]))
    for copy in outs:
        copy.wait()
    arrive(small_hbm.at[1:], small_recv.at[1], "sp")


def hand_over_kernel(
    values_hbm, gates_hbm, weight_hbm, small_hbm,
    values_grad_hbm, gates_grad_hbm, weight_grad_hbm, taps_grad_hbm, gain_grad_hbm, bias_grad_hbm,
    values, gates, weight, small, taps_grad, gain_grad, bias_grad, in_sems, out_sems,
):
    seqs = values.shape[0]
    pairs = [(small_hbm, small, None)]
    for s in range(seqs):
        pairs.append((values_hbm.at[s], values.at[s], values_grad_hbm.at[s]))
        pairs.append((gates_hbm.at[s], gates.at[s], gates_grad_hbm.at[s]))
    pairs.append((weight_hbm, weight, weight_grad_hbm))
    loads = [
        pltpu.make_async_copy(src, here, in_sems.at[n]) for n, (src, here, _) in enumerate(pairs)
    ]
    for copy in loads:
        copy.start()
    stores = []

    def store(here, dst):
        stores.append(pltpu.make_async_copy(here, dst, out_sems.at[len(stores)]))
        stores[-1].start()

    for copy, (_, here, dst) in zip(loads[1:], pairs[1:]):
        copy.wait()
        store(here, dst)
    loads[0].wait()
    total = small[0].astype(F32)
    for d in range(1, small.shape[0]):
        total = total + small[d].astype(F32)
    taps_grad[...] = total[:K]
    bias_grad[...] = total[32:33]
    gain_grad[...] = total[33:34]
    store(taps_grad, taps_grad_hbm)
    store(gain_grad, gain_grad_hbm)
    store(bias_grad, bias_grad_hbm)
    for copy in stores:
        copy.wait()


def on_device(values_in, gates_in, conv_taps, conv_bias, norm_gain, out_weight, out_grad):
    seqs, tokens, chans = values_in.shape
    width = out_grad.shape[2]
    total_chans = chans * lax.axis_size("tp")
    positions = seqs * tokens
    rows = min(512, tokens)
    blocks = positions // rows
    chunks = tokens // LANES
    windows = -(-tokens // STEP)
    strips = 8
    parts = 16
    tp_others = lax.axis_size("tp") - 1
    sp_devices = lax.axis_size("sp")
    groups = sp_devices // PAIR
    weight_rows = chans // sp_devices
    small_rows = 48

    def dma(*shape):
        return pltpu.SemaphoreType.DMA(shape)

    one = pltpu.SemaphoreType.DMA
    anywhere = pl.BlockSpec(memory_space=pl.ANY)
    padded = windows * STEP + HALO
    block_sums = (2, rows // LANES, LANES)
    values_sum, gates_sum, small, weight_sum = pl.pallas_call(
        functools.partial(fused_kernel, total_chans),
        in_specs=[anywhere] * 8,
        out_specs=[anywhere] * 4,
        out_shape=[
            jax.ShapeDtypeStruct((seqs, tokens, chans), BF16),
            jax.ShapeDtypeStruct((seqs, tokens, chans), BF16),
            jax.ShapeDtypeStruct((groups, small_rows, chans), BF16),
            jax.ShapeDtypeStruct((weight_rows, width), F32),
        ],
        scratch_shapes=[
            pltpu.VMEM((seqs, tokens, chans), BF16),
            pltpu.VMEM((seqs, tokens, chans), BF16),
            pltpu.VMEM((seqs, HALO, chans), BF16),
            pltpu.VMEM((seqs, HALO, chans), BF16),
            pltpu.VMEM((positions, width), BF16),
            pltpu.VMEM((chans, max(positions, width)), BF16),
            pltpu.VMEM((width, chans), BF16),
            pltpu.VMEM((PAIR, groups, weight_rows, width), BF16),
            pltpu.VMEM((groups, weight_rows, width), BF16),
            pltpu.VMEM((groups - 1, weight_rows, width), BF16),
            pltpu.VMEM((groups - 1, weight_rows, width), BF16),
            pltpu.VMEM((weight_rows, width), F32),
            pltpu.VMEM((seqs, tokens, chans), F32),
            pltpu.VMEM((seqs, tokens, chans), F32),
            pltpu.VMEM((2, rows, chans), F32),
            pltpu.VMEM((seqs, SPAN, chans), BF16),
            pltpu.VMEM((SPAN, chans), BF16),
            pltpu.VMEM((seqs * windows, SPAN, chans), BF16),
            pltpu.VMEM((windows, SPAN, chans), BF16),
            pltpu.VMEM((windows, SPAN, chans), BF16),
            pltpu.VMEM((padded, chans), BF16),
            pltpu.VMEM((padded, chans), BF16),
            pltpu.VMEM((TABLE_ROWS, SPAN), BF16),
            pltpu.VMEM((K, chans), BF16),
            pltpu.VMEM((chans,), BF16),
            pltpu.VMEM((chans,), BF16),
            pltpu.VMEM((SPAN, chans), F32),
            pltpu.VMEM((SPAN // 2, chans), F32),
            pltpu.VMEM((SPAN // 2, chans), F32),
            pltpu.VMEM((SPAN // 2, chans), F32),
            pltpu.VMEM((SPAN // 2, chans), F32),
            pltpu.VMEM((seqs, HALO, chans), BF16),
            pltpu.VMEM((seqs, HALO, chans), BF16),
            pltpu.VMEM((seqs, 2, chunks, LANES), F32),
            pltpu.VMEM((tp_others, seqs, 2, chunks, LANES), F32),
            pltpu.VMEM((seqs, chunks, LANES), F32),
            pltpu.VMEM((blocks, *block_sums), F32),
            pltpu.VMEM((tp_others, blocks, *block_sums), F32),
            pltpu.VMEM((8, chans), F32),
            pltpu.VMEM((8, chans), F32),
            pltpu.VMEM((small_rows, chans), F32),
            pltpu.VMEM((small_rows, chans), BF16),
            pltpu.VMEM((small_rows, chans), F32),
            dma(2, seqs),
            dma(strips),
            dma(5),
            dma(2),
            dma(2, seqs),
            one,
            dma(seqs),
            one,
            dma(seqs),
            one,
            dma(parts),
            one,
            one,
            one,
            one,
            one,
            dma(2),
        ],
        compiler_params=pltpu.CompilerParams(
            vmem_limit_bytes=VMEM_LIMIT, collective_id=0, has_side_effects=True
        ),
        name="fused",
    )(
        values_in, gates_in, out_grad.reshape(positions, width), out_weight,
        jnp.asarray(transform_table()), conv_taps, conv_bias, norm_gain,
    )

    values_grad, gates_grad, weight_grad, taps_grad, gain_grad, bias_grad = pl.pallas_call(
        hand_over_kernel,
        in_specs=[anywhere] * 4,
        out_specs=[anywhere] * 6,
        out_shape=[
            jax.ShapeDtypeStruct((seqs, tokens, chans), BF16),
            jax.ShapeDtypeStruct((seqs, tokens, chans), BF16),
            jax.ShapeDtypeStruct((weight_rows, width), F32),
            jax.ShapeDtypeStruct((K, chans), F32),
            jax.ShapeDtypeStruct((1, chans), F32),
            jax.ShapeDtypeStruct((1, chans), F32),
        ],
        scratch_shapes=[
            pltpu.VMEM((seqs, tokens, chans), BF16),
            pltpu.VMEM((seqs, tokens, chans), BF16),
            pltpu.VMEM((weight_rows, width), F32),
            pltpu.VMEM((groups, small_rows, chans), BF16),
            pltpu.VMEM((K, chans), F32),
            pltpu.VMEM((1, chans), F32),
            pltpu.VMEM((1, chans), F32),
            dma(2 * seqs + 2),
            dma(2 * seqs + 4),
        ],
        compiler_params=pltpu.CompilerParams(vmem_limit_bytes=VMEM_LIMIT),
        name="hand_over",
    )(values_sum, gates_sum, weight_sum, small)
    return values_grad, gates_grad, taps_grad, gain_grad[0], bias_grad[0], weight_grad


def solution(mesh):
    return jax.shard_map(
        on_device,
        mesh=mesh,
        in_specs=(
            P(None, "sp", "tp"),
            P(None, "sp", "tp"),
            P(None, "tp"),
            P("tp"),
            P("tp"),
            P("tp", None),
            P(None, "sp", None),
        ),
        out_specs=(
            P(None, "sp", "tp"),
            P(None, "sp", "tp"),
            P(None, "tp"),
            P("tp"),
            P("tp"),
            P(("tp", "sp"), None),
        ),
        check_vma=False,
    )
```
